256 devices in a mesh: sp: 64 (over z, y, core), tp: 4 (over x).
Axes of the slice: x: 4, y: 4, z: 8, core: 2. Of those that a mesh axis runs over, the one named last changes fastest.
Arguments:
- resid_in: bfloat16 [16384, 2048], P(('sp', 'tp')), may hold values from -6 to 6
- query_proj: bfloat16 [16384, 512], P('sp', 'tp'), may hold values from -6 to 6
- key_proj: bfloat16 [16384, 256], P('sp', 'tp'), may hold values from -6 to 6
- value_proj: bfloat16 [16384, 256], P('sp', 'tp'), may hold values from -6 to 6
- query_gain: float32 [8, 64], P('tp'), may hold values from 0.5 to 6
- key_gain: float32 [4, 64], P('tp'), may hold values from 0.5 to 6
- out_weight: bfloat16 [512, 2048], replicated, may hold values from -0.25 to 0.25
- norm_gain: float32 [2048], replicated, may hold values from 0.1 to 1.9
- gate_weight: bfloat16 [64, 2048, 1024], P('sp', None, 'tp'), may hold values from -0.125 to 0.125
- up_weight: bfloat16 [64, 2048, 1024], P('sp', None, 'tp'), may hold values from -0.125 to 0.125
- down_weight: bfloat16 [64, 1024, 2048], P('sp', 'tp'), may hold values from -0.1875 to 0.1875
- expert_ids: int32 [16384, 2], P('sp'), may hold values from 0 to 63, all different within a row; in each aligned block of 64 rows (0 to 63, 64 to 127, ...) at most 3 rows name the same one
- route_weight: float32 [16384, 2], P(('sp', 'tp')), may hold values from 0.2 to 1
Outputs:
- layer_out: bfloat16 [16384, 2048], P(('sp', 'tp'))
The draws below stay inside these ranges and needn't reach their ends.
Inputs may be any that keep to these rules, and one draw needn't show every extreme that they name: `expert_ids`: each row names 2 different experts. In each aligned block of rows that one device holds (rows of one index of sp and tp together), no expert is named more than 3 times, and in some blocks one expert is named exactly 3 times.
All inputs are finite; a program needn't handle non-finite values.
Results may differ from the reference program's by a relative error of at most 0.014.
Values may be sent and summed in bfloat16 or wider, within the bound.
A program may use at most 64 MiB of HBM per device.

```python
import math
import jax
import jax.numpy as jnp
import numpy as np
from jax import lax

D = 2048
HEADS = 8
KV_HEADS = 4
HEAD_DIM = 64
FF = 1024
TOPK = 2
GRID_W = 64
TOK_DEV = 256
TOKENS = 16384
EXPERTS = 64
A_WIDTH = 512
FF_DEV = 256
CAP = 3
N_TP = 4


def drawn_pair(key):
    folded = jax.random.fold_in(key, 31)
    query_key, other_key = jax.random.split(folded, 2)
    queries = jnp.clip(jax.random.normal(query_key, (TOKENS, HEADS * HEAD_DIM), jnp.float32), -6.0, 6.0)
    keys_drawn = jnp.clip(jax.random.normal(other_key, (TOKENS, KV_HEADS * HEAD_DIM), jnp.float32), -6.0, 6.0)
    return (queries, keys_drawn)


def draw_query_proj(key, part):
    return drawn_pair(key)[0].astype(jnp.bfloat16)


def draw_key_proj(key, part):
    return drawn_pair(key)[1].astype(jnp.bfloat16)


def gain_table(key, head_count, salt):
    folded = jax.random.fold_in(key, salt)
    first_key = jax.random.fold_in(folded, 0)
    return jax.random.uniform(first_key, (head_count, HEAD_DIM), jnp.float32, 0.5, 2.0)


def draw_query_gain(key, part):
    return gain_table(key, HEADS, 5)


def draw_key_gain(key, part):
    return gain_table(key, KV_HEADS, 9)


def block_scale(stream_key, extent, cuts, smallest, largest):
    factor_of, own = 1.0, jax.random.fold_in(stream_key, 6)
    for position, parts in cuts:
        steps = jnp.exp(jax.random.uniform(jax.random.fold_in(own, position), (parts,), jnp.float32, smallest / len(cuts), largest / len(cuts)))
        factor_of = factor_of * jnp.repeat(steps, extent[position] // parts).reshape([-1 if axis == position else 1 for axis in range(len(extent))])
    return factor_of


def shared_out(own_key, own, number, rows, count, top, most, slope):
    sequence = jax.random.permutation(own_key, count)
    crowded, usual = shares(count, rows * top, most, slope, True), shares(count, rows * top, most, slope, False)
    places = jnp.arange(count)

    def named(tallies, rotation):
        used = int((tallies > 0).sum())
        fixed = max(1, used // 4)
        passed = fixed + (places - fixed + rotation * (used - fixed)) % max(1, count - fixed)
        return jnp.zeros((count,), jnp.int32).at[sequence[jnp.where(places < fixed, places, passed)]].set(jnp.asarray(tallies, jnp.int32))

    tallies = jnp.where(number % 4 == 0, named(crowded, number // 4), named(usual, number - number // 4 - 1))
    mixed = jax.random.permutation(jax.random.fold_in(own, 3), count)
    giver, taker = mixed[0:count // 2 * 2:2], mixed[1:count // 2 * 2:2]
    margin = jnp.minimum(tallies[giver] - 1, most - tallies[taker]) // 2
    margin = jnp.where((giver == sequence[0]) | (taker == sequence[0]) | (tallies[taker] == 0), 0, jnp.maximum(margin, 0))
    passed = jax.random.randint(jax.random.fold_in(own, 4), (count // 2,), 0, 1 << 20) % (margin + 1)
    tallies = tallies.at[giver].add(-passed).at[taker].add(passed)
    items = jnp.searchsorted(jnp.cumsum(tallies), jnp.arange(rows * top), side="right").astype(jnp.int32)
    table = items.reshape(top, rows).T
    table = table[jax.random.permutation(jax.random.fold_in(own, 1), rows)]
    rotation = jax.random.randint(jax.random.fold_in(own, 2), (rows, 1), 0, top)
    return jnp.take_along_axis(table, (jnp.arange(top)[None, :] + rotation) % top, axis=1)


def shares(count, total, bound, slope, full):
    portions = [(1 << 20) // math.isqrt(standing ** slope) + 1 for standing in range(1, count + 1)]
    largest = bound if full else min(bound, max(-(-total // count), total * portions[0] // sum(portions)))
    least = 1 if total - largest >= count - 1 else 0
    holding, surplus = [largest] + [least] * (count - 1), total - largest - least * (count - 1)
    while surplus > 0:
        candidates = [i for i in range(1, count) if holding[i] < largest] or [i for i in range(1, count) if holding[i] < bound]
        mass, budget = sum([portions[i] for i in candidates]), surplus
        for i in candidates:
            addition = min(bound - holding[i], max(1, budget * portions[i] // mass), surplus)
            holding[i] = holding[i] + addition
            surplus = surplus - addition
    return np.array(holding)


def centred(own_key, shape, deviation, limit, cuts=(), kind=jnp.bfloat16):
    array = jax.random.normal(own_key, shape, jnp.float32) * deviation
    if len(cuts) > 0:
        array = block_scale(own_key, shape, cuts, -0.22, 0.18) * array
    return jnp.clip(array, min=-limit, max=limit).astype(kind)


def setup_inputs(seed: int = 0) -> dict:
    key_of = jax.random.split(jax.random.key(seed), 14)
    resid_in = centred(key_of[0], (TOKENS, D), 1.0, 6.0, ((0, 256),))
    query_proj = draw_query_proj(jax.random.fold_in(key_of[13], 71), 0)
    key_proj = draw_key_proj(jax.random.fold_in(key_of[13], 71), 0)
    value_proj = centred(key_of[3], (TOKENS, KV_HEADS * HEAD_DIM), 1.0, 6.0, ((0, 64), (1, 4)))
    query_gain = draw_query_gain(jax.random.fold_in(key_of[13], 71), 0)
    key_gain = draw_key_gain(jax.random.fold_in(key_of[13], 71), 0)
    out_weight = centred(key_of[6], (A_WIDTH, D), A_WIDTH ** -0.5, 0.25)
    norm_gain = jnp.clip(1.0 + 0.18 * jax.random.normal(key_of[7], (D,), jnp.float32), 0.1, 1.9)
    gate_weight = centred(key_of[8], (EXPERTS, D, FF), D ** -0.5, 0.125, ((0, 64), (2, 4)))
    up_weight = centred(key_of[9], (EXPERTS, D, FF), D ** -0.5, 0.125, ((0, 64), (2, 4)))
    down_weight = centred(key_of[10], (EXPERTS, FF, D), FF ** -0.5, 0.1875, ((0, 64), (1, 4)))
    expert_ids_keys = jax.random.split(jax.random.fold_in(key_of[11], 1), TOKENS // (TOK_DEV // N_TP))
    expert_ids_turns = jax.random.permutation(jax.random.fold_in(key_of[11], 3), TOKENS // (TOK_DEV // N_TP))
    expert_ids = jax.vmap(lambda own, number: shared_out(jax.random.fold_in(key_of[11], 2), own, number, TOK_DEV // N_TP, EXPERTS, TOPK, CAP, 1))(expert_ids_keys, expert_ids_turns).reshape((TOKENS, TOPK))
    route_weight = jnp.clip(0.2 + 0.8 * jax.random.uniform(key_of[12], (TOKENS, TOPK), jnp.float32) ** block_scale(key_of[12], (TOKENS, TOPK), ((0, 256),), -0.2, 0.2), 0.2, 1.0)
    return {"resid_in": resid_in, "query_proj": query_proj, "key_proj": key_proj, "value_proj": value_proj, "query_gain": query_gain, "key_gain": key_gain, "out_weight": out_weight, "norm_gain": norm_gain, "gate_weight": gate_weight, "up_weight": up_weight, "down_weight": down_weight, "expert_ids": expert_ids, "route_weight": route_weight}


eps = 1e-06
rope_base = 10000.0
query_block = 64

def rotary_tables(positions):
    row_pos = (positions // GRID_W).astype(jnp.float32)
    col_pos = (positions % GRID_W).astype(jnp.float32)
    freq_count = HEAD_DIM // 4
    inverse = rope_base ** (-jnp.arange(freq_count, dtype=jnp.float32) / freq_count)
    angles = jnp.concatenate([row_pos[:, None] * inverse, col_pos[:, None] * inverse], axis=-1)
    return (jnp.cos(angles), jnp.sin(angles))

def prepare(projected, gains, cosine, sine_table):
    tok_total = projected.shape[0]
    head_count = gains.shape[0]
    values_f = projected.astype(jnp.float32).reshape(tok_total, head_count, HEAD_DIM)
    normed = values_f * lax.rsqrt(lax.optimization_barrier(jnp.mean(values_f * values_f, axis=-1, keepdims=True)) + eps) * gains[None]
    half_dim = HEAD_DIM // 2
    first_half = normed[..., :half_dim]
    second_half = normed[..., half_dim:]
    cos_b = cosine[:, None, :]
    sin_b = sine_table[:, None, :]
    rotated = jnp.concatenate([first_half * cos_b - second_half * sin_b, second_half * cos_b + first_half * sin_b], axis=-1)
    return rotated.astype(jnp.bfloat16)

def reference(resid_in, query_proj, key_proj, value_proj, query_gain, key_gain, out_weight, norm_gain, gate_weight, up_weight, down_weight, expert_ids, route_weight):
    positions = jnp.arange(TOKENS, dtype=jnp.int32)
    cosine, sine_table = rotary_tables(positions)
    query_rot = prepare(query_proj, query_gain, cosine, sine_table)
    key_rot = prepare(key_proj, key_gain, cosine, sine_table)
    group_size = HEADS // KV_HEADS
    grouped = query_rot.reshape(TOKENS // query_block, query_block, KV_HEADS, group_size, HEAD_DIM)
    key_f = key_rot.astype(jnp.float32)
    value_f = value_proj.reshape(TOKENS, KV_HEADS, HEAD_DIM).astype(jnp.float32)

    def attend_block(block_q):
        scores = jnp.einsum('qkgd,skd->qkgs', block_q.astype(jnp.float32), key_f) * HEAD_DIM ** (-0.5)
        row_max = lax.optimization_barrier(jnp.max(scores, axis=-1, keepdims=True))
        exponents = jnp.exp(scores - row_max)
        weights = exponents.astype(jnp.bfloat16)
        row_sum = lax.optimization_barrier(jnp.sum(exponents, axis=-1))
        summed_values = jnp.einsum('qkgs,skd->qkgd', weights.astype(jnp.float32), value_f)
        return (summed_values / row_sum[..., None]).astype(jnp.bfloat16)
    attended = lax.map(attend_block, grouped).reshape(TOKENS, HEADS * HEAD_DIM)
    mixed_out = jnp.dot(attended, out_weight, preferred_element_type=jnp.float32)
    residual = (resid_in.astype(jnp.float32) + mixed_out).astype(jnp.bfloat16)
    resid_f = residual.astype(jnp.float32)
    normed = (resid_f * lax.rsqrt(lax.optimization_barrier(jnp.mean(resid_f * resid_f, axis=-1, keepdims=True)) + eps) * norm_gain).astype(jnp.bfloat16)
    block_rows = TOK_DEV // N_TP
    n_blocks = TOKENS // block_rows
    ids_blocks = expert_ids.reshape(n_blocks, block_rows * TOPK).astype(jnp.int32)
    member = (ids_blocks[:, :, None] == jnp.arange(EXPERTS, dtype=jnp.int32)[None, None, :]).astype(jnp.int32)
    ranks = lax.optimization_barrier(jnp.sum((jnp.cumsum(member, axis=1) - member) * member, axis=2))
    block_index = jnp.arange(n_blocks, dtype=jnp.int32)[:, None]
    slot_pos = (block_index * CAP + ranks).astype(jnp.int32)
    token_of = jnp.repeat(jnp.arange(TOKENS, dtype=jnp.int32), TOPK).reshape(n_blocks, block_rows * TOPK)
    row_table = jnp.full((EXPERTS, n_blocks * CAP), TOKENS, jnp.int32).at[ids_blocks, slot_pos].set(token_of)
    normed_pad = jnp.concatenate([normed, jnp.zeros((1, D), jnp.bfloat16)], axis=0)

    def run_expert(args):
        table_row, gate_e, up_e, down_e = args
        rows = normed_pad[table_row]
        gate = jnp.dot(rows, gate_e, preferred_element_type=jnp.float32)
        upper = jnp.dot(rows, up_e, preferred_element_type=jnp.float32)
        hidden = (jax.nn.silu(gate) * upper).astype(jnp.bfloat16)
        accum = jnp.zeros((rows.shape[0], D), jnp.float32)
        for block_index_ff in range(FF // FF_DEV):
            lower = block_index_ff * FF_DEV
            partial_value = jnp.dot(hidden[:, lower:lower + FF_DEV], down_e[lower:lower + FF_DEV], preferred_element_type=jnp.float32)
            accum = accum + lax.optimization_barrier(partial_value.astype(jnp.bfloat16)).astype(jnp.float32)
        return accum.astype(jnp.bfloat16)
    outputs_all = lax.map(run_expert, (row_table, gate_weight, up_weight, down_weight))
    picked = outputs_all[ids_blocks, slot_pos].reshape(TOKENS, TOPK, D).astype(jnp.float32)
    combined = lax.optimization_barrier(jnp.sum(picked * route_weight[:, :, None], axis=1))
    return (resid_f + combined).astype(jnp.bfloat16)
```

```python
import functools

import jax
import jax.numpy as jnp
from jax import lax
from jax.experimental import pallas as pl
from jax.experimental.pallas import tpu as pltpu
from jax.sharding import PartitionSpec as P

HEAD_DIM = 64
TOPK = 2
GRID_W = 64
TOK_DEV = 256


eps = 1e-06
rope_base = 10000.0


def joined_along(tiles, dim):
    dims = list(tiles.shape[1:])
    dims[dim] *= tiles.shape[0]
    return jnp.moveaxis(tiles, 0, dim).reshape(dims)


def work_in_pieces(value, axis, dim, apply, out_dim):
    devices, width = (lax.axis_size(axis), value.shape[dim])
    count = 2 if width % 2 == 0 else 1
    gathered, length = ([], width // count)
    for k in range(count):
        piece = lax.slice_in_dim(value, k * length, (k + 1) * length, axis=dim)
        starts = jnp.arange(devices) * width + k * length
        gathered.append(jax.vmap(apply)(lax.all_gather(piece, axis), starts))
    return joined_along(jnp.concatenate(gathered, axis=out_dim + 1), out_dim)


def in_blocks(value, dim, devices):
    before, after = (value.shape[:dim], value.shape[dim + 1 :])
    return jnp.moveaxis(value.reshape(*before, devices, -1, *after), dim, 0)


def summed_on_arrival(value, axis, dim):
    devices = lax.axis_size(axis)
    tiles = lax.all_to_all(in_blocks(value, dim, devices), axis, 0, 0, tiled=True)
    return jnp.sum(tiles.astype(jnp.float32), axis=0)


def rotary_tables(positions):
    row_pos = (positions // GRID_W).astype(jnp.float32)
    col_pos = (positions % GRID_W).astype(jnp.float32)
    freq_count = HEAD_DIM // 4
    inverse = rope_base ** (-jnp.arange(freq_count, dtype=jnp.float32) / freq_count)
    angles = jnp.concatenate([row_pos[:, None] * inverse, col_pos[:, None] * inverse], axis=-1)
    return (jnp.cos(angles), jnp.sin(angles))


def prepare(projected, gains, cosine, sine_table):
    tok_total = projected.shape[0]
    head_count = gains.shape[0]
    values_f = projected.astype(jnp.float32).reshape(tok_total, head_count, HEAD_DIM)
    normed = (
        values_f
        * lax.rsqrt(jnp.mean(values_f * values_f, axis=-1, keepdims=True) + eps)
        * gains[None]
    )
    half_dim = HEAD_DIM // 2
    first_half = normed[..., :half_dim]
    second_half = normed[..., half_dim:]
    cos_b = cosine[:, None, :]
    sin_b = sine_table[:, None, :]
    rotated = jnp.concatenate(
        [first_half * cos_b - second_half * sin_b, second_half * cos_b + first_half * sin_b],
        axis=-1,
    )
    return rotated.astype(jnp.bfloat16)


def slot_index(ids_rows, expert_count, capacity):
    flat_ids = ids_rows.reshape(-1)
    member = (flat_ids[:, None] == jnp.arange(expert_count, dtype=jnp.int32)[None, :]).astype(
        jnp.int32
    )
    ranks = jnp.sum((jnp.cumsum(member, axis=0) - member) * member, axis=1)
    return flat_ids * capacity + ranks


def build_send(rows, ids_rows, expert_count, capacity):
    slot_ids = slot_index(ids_rows, expert_count, capacity)
    picker = (
        jnp.arange(expert_count * capacity, dtype=jnp.int32)[:, None] == slot_ids[None, :]
    ).astype(jnp.bfloat16)
    repeated = jnp.repeat(rows, ids_rows.shape[1], axis=0)
    outgoing = jnp.dot(picker, repeated, preferred_element_type=jnp.float32).astype(jnp.bfloat16)
    return outgoing.reshape(expert_count, capacity, rows.shape[1])


def expert_ffn(rows, gate_local, up_local, down_local):
    lead_shape = rows.shape[:-1]
    flat_rows = rows.reshape(-1, rows.shape[-1])
    gate = jnp.dot(flat_rows, gate_local, preferred_element_type=jnp.float32)
    upper = jnp.dot(flat_rows, up_local, preferred_element_type=jnp.float32)
    hidden = (jax.nn.silu(gate) * upper).astype(jnp.bfloat16)
    result = jnp.dot(hidden, down_local, preferred_element_type=jnp.float32)
    return result.reshape(lead_shape + (down_local.shape[1],))


LANES = 128
MESH = pl.DeviceIdType.MESH
LOG2E = 1.4426950408889634


def attention_kernel(
    q_ref, kv_ref, out_ref,
    qall, kvall, kk, vt, osend, mlsend, orecv, mlrecv, own_o, own_ml, attv,
    qs, qr, ks, kr, os_, or_, ms, mr, xs, xr,
):
    sp = lax.axis_index("sp")
    me_x = lax.axis_index("tp")
    z, j = sp // 8, sp % 8
    tok = q_ref.shape[0]

    def group(d):
        return z * 8 + lax.rem(j + d, 8)

    def ring(d):
        return lax.rem(z + d, 8) * 8 + j

    barrier = pltpu.get_barrier_semaphore()
    for d in range(1, 8):
        pl.semaphore_signal(barrier, inc=1, device_id=(group(d), me_x), device_id_type=MESH)
        pl.semaphore_signal(barrier, inc=1, device_id=(ring(d), me_x), device_id_type=MESH)
    for d in range(1, 4):
        pl.semaphore_signal(barrier, inc=1, device_id=(sp, lax.rem(me_x + d, 4)), device_id_type=MESH)
    pl.semaphore_wait(barrier, 17)

    def q_copy(d):
        return pltpu.make_async_remote_copy(
            src_ref=q_ref, dst_ref=qall.at[d], send_sem=qs.at[d], recv_sem=qr.at[d],
            device_id=(group(d), me_x), device_id_type=MESH)

    def kv_copy(d):
        return pltpu.make_async_remote_copy(
            src_ref=kv_ref, dst_ref=kvall.at[d], send_sem=ks.at[d], recv_sem=kr.at[d],
            device_id=(ring(d), me_x), device_id_type=MESH)

    order = (4, 3, 5, 2, 6, 1, 7)
    for d in order:
        q_copy(d).start()
        kv_copy(d).start()

    lane = lax.broadcasted_iota(jnp.int32, (tok, LANES), 1)
    low = lane < HEAD_DIM

    def spread(block, at):
        f = block.astype(jnp.float32)
        kk[pl.ds(at * tok, tok), :] = jnp.where(low, f, pltpu.roll(f, HEAD_DIM, 1)).astype(jnp.bfloat16)
        t = f.T.astype(jnp.bfloat16)
        vt[0:HEAD_DIM, at * tok:(at + 1) * tok] = t[HEAD_DIM:, :]

    vt[HEAD_DIM:, :] = jnp.ones((16, vt.shape[1]), jnp.bfloat16)
    qall[0] = q_ref[...]
    spread(kv_ref[...], 0)
    for d in (1, 7, 2, 6, 3, 5, 4):
        kv_copy(d).wait()
        spread(kvall[d], d)
    for d in range(1, 8):
        q_copy(d).wait()

    chunk = 512
    factor = LOG2E * HEAD_DIM ** (-0.5)

    def o_copy(d):
        return pltpu.make_async_remote_copy(
            src_ref=osend.at[d], dst_ref=orecv.at[d], send_sem=os_.at[d], recv_sem=or_.at[d],
            device_id=(group(8 - d), me_x), device_id_type=MESH)

    def ml_copy(d):
        return pltpu.make_async_remote_copy(
            src_ref=mlsend.at[d], dst_ref=mlrecv.at[d], send_sem=ms.at[d], recv_sem=mr.at[d],
            device_id=(group(8 - d), me_x), device_id_type=MESH)

    def block_of(q):
        zero = jnp.zeros_like(q)
        both = jnp.concatenate([jnp.where(low, q, zero), jnp.where(low, zero, q)], axis=0)
        best = acc = None
        for c in range(8 * tok // chunk):
            keys = kk[c * chunk:(c + 1) * chunk, :]
            s = lax.dot_general(keys, both, (((1,), (1,)), ((), ())), preferred_element_type=jnp.float32)
            top = jnp.max(s, axis=0, keepdims=True)
            new = top if best is None else jnp.maximum(best, top)
            p = jnp.exp2((s - new) * factor).astype(jnp.bfloat16)
            part = jnp.dot(vt[:, c * chunk:(c + 1) * chunk], p, preferred_element_type=jnp.float32)
            acc = part if best is None else acc * jnp.exp2((best - new) * factor) + part
            best = new
        return best, acc

    def put(o_ref, ml_ref, best, acc):
        o_ref[0:HEAD_DIM, :] = acc[0:HEAD_DIM, 0:tok].astype(o_ref.dtype)
        o_ref[HEAD_DIM:, :] = acc[0:HEAD_DIM, tok:].astype(o_ref.dtype)
        ml_ref[0:1, :] = best
        ml_ref[1:2, :] = acc[HEAD_DIM:HEAD_DIM + 1, :]

    def step(d, carry):
        best, acc = block_of(qall[d])
        put(osend.at[d], mlsend.at[d], best, acc)
        o_copy(d).start()
        ml_copy(d).start()
        return carry

    lax.fori_loop(1, 8, step, 0)
    best, acc = block_of(qall[0])
    put(own_o, own_ml, best, acc)

    def finish(d, carry):
        ml_copy(d).wait()
        o_copy(d).wait()
        return carry

    lax.fori_loop(1, 8, finish, 0)
    tops = [own_ml[0:1, :]] + [mlrecv[d, 0:1, :] for d in range(1, 8)]
    top = functools.reduce(jnp.maximum, tops)
    sums = jnp.zeros_like(top)
    heads = [jnp.zeros((HEAD_DIM, tok), jnp.float32) for _ in range(2)]
    for d in range(8):
        w = jnp.exp2((tops[d] - top) * factor)
        sums = sums + w * (own_ml[1:2, :] if d == 0 else mlrecv[d, 1:2, :])
        o = own_o[...] if d == 0 else orecv[d].astype(jnp.float32)
        for h in range(2):
            heads[h] = heads[h] + o[h * HEAD_DIM:(h + 1) * HEAD_DIM, :] * w[:, h * tok:(h + 1) * tok]
    full = jnp.concatenate([heads[h] / sums[:, h * tok:(h + 1) * tok] for h in range(2)], axis=0)
    rows = full.T.astype(jnp.bfloat16)
    own_rows = tok // 4
    for x in range(4):
        attv[x] = rows[x * own_rows:(x + 1) * own_rows, :]

    def x_copy(d):
        return pltpu.make_async_remote_copy(
            src_ref=attv.at[lax.rem(me_x + d, 4)], dst_ref=out_ref.at[me_x],
            send_sem=xs.at[d], recv_sem=xr.at[d],
            device_id=(sp, lax.rem(me_x + d, 4)), device_id_type=MESH)

    for d in (2, 1, 3):
        x_copy(d).start()
    out_ref[me_x] = attv[me_x]
    for d in (1, 3, 2):
        x_copy(d).wait()


def attention(q, kv):
    tok = q.shape[0]
    bf, f32 = jnp.bfloat16, jnp.float32
    dma = pltpu.SemaphoreType.DMA
    return pl.pallas_call(
        attention_kernel,
        out_shape=jax.ShapeDtypeStruct((4, tok // 4, LANES), bf),
        in_specs=[pl.BlockSpec(memory_space=pltpu.VMEM)] * 2,
        out_specs=pl.BlockSpec(memory_space=pltpu.VMEM),
        scratch_shapes=[
            pltpu.VMEM((8, tok, LANES), bf),
            pltpu.VMEM((8, tok, LANES), bf),
            pltpu.VMEM((8 * tok, LANES), bf),
            pltpu.VMEM((HEAD_DIM + 16, 8 * tok), bf),
            pltpu.VMEM((8, LANES, tok), bf),
            pltpu.VMEM((8, 2, 2 * tok), f32),
            pltpu.VMEM((8, LANES, tok), bf),
            pltpu.VMEM((8, 2, 2 * tok), f32),
            pltpu.VMEM((LANES, tok), f32),
            pltpu.VMEM((2, 2 * tok), f32),
            pltpu.VMEM((4, tok // 4, LANES), bf),
        ] + [dma((8,))] * 8 + [dma((4,))] * 2,
        compiler_params=pltpu.CompilerParams(
            collective_id=0, has_side_effects=True, vmem_limit_bytes=48 << 20),
        cost_estimate=pl.CostEstimate(flops=4 * 8 * tok * 8 * tok * 2 * HEAD_DIM, bytes_accessed=1 << 20, transcendentals=0),
    )(q, kv)


def body(
    resid_in,
    query_proj,
    key_proj,
    value_proj,
    query_gain,
    key_gain,
    out_weight,
    norm_gain,
    gate_weight,
    up_weight,
    down_weight,
    expert_ids,
    route_weight,
):
    tok_count = query_proj.shape[0]
    head_local = query_gain.shape[0]
    positions = lax.axis_index("sp") * tok_count + lax.iota(jnp.int32, tok_count)
    cosine, sine_table = rotary_tables(positions)
    query_rot = prepare(query_proj, query_gain, cosine, sine_table)
    key_rot = prepare(key_proj, key_gain, cosine, sine_table)
    regrouped = attention(
        query_rot.reshape(tok_count, head_local * HEAD_DIM),
        jnp.concatenate([key_rot.reshape(tok_count, HEAD_DIM), value_proj], axis=1),
    )
    tp_count = lax.axis_size("tp")
    row_count = tok_count // tp_count
    mixed_out = jnp.einsum(
        "xtd,xdo->to", regrouped, out_weight.reshape(tp_count, -1, out_weight.shape[1]),
        preferred_element_type=jnp.float32,
    )
    residual = (resid_in.astype(jnp.float32) + mixed_out).astype(jnp.bfloat16)
    resid_f = residual.astype(jnp.float32)
    normed = (
        resid_f * lax.rsqrt(jnp.mean(resid_f * resid_f, axis=-1, keepdims=True) + eps) * norm_gain
    ).astype(jnp.bfloat16)
    expert_count = lax.axis_size("sp")
    capacity = max(2, 3 * TOPK * TOK_DEV // (2 * tp_count * expert_count))
    own_ids = lax.dynamic_slice_in_dim(expert_ids, lax.axis_index("tp") * row_count, row_count, 0)
    slot_ids = slot_index(own_ids, expert_count, capacity)
    gate_local = gate_weight[0]
    up_local = up_weight[0]
    down_local = down_weight[0]
    outgoing = build_send(normed, own_ids, expert_count, capacity)
    received = lax.all_to_all(outgoing, "sp", split_axis=0, concat_axis=0, tiled=True)

    def expert_rows(segment, begin_row):
        return expert_ffn(segment, gate_local, up_local, down_local)

    partial_value = work_in_pieces(received[None], "tp", 0, expert_rows, 0)
    summed = summed_on_arrival(partial_value.astype(jnp.bfloat16), "tp", 0)
    expert_out = summed[0].astype(jnp.bfloat16)
    returned = lax.all_to_all(expert_out, "sp", split_axis=0, concat_axis=0, tiled=True)
    flat_out = returned.reshape(expert_count * capacity, returned.shape[-1])
    picked = (
        jnp.take(flat_out, slot_ids, axis=0)
        .astype(jnp.float32)
        .reshape(row_count, route_weight.shape[1], flat_out.shape[1])
    )
    combined = jnp.sum(picked * route_weight[:, :, None], axis=1)
    return (resid_f + combined).astype(jnp.bfloat16)


def solution(mesh):
    placed = (
        P(("sp", "tp"), None),
        P("sp", "tp"),
        P("sp", "tp"),
        P("sp", "tp"),
        P("tp", None),
        P("tp", None),
        P(),
        P(),
        P("sp", None, "tp"),
        P("sp", None, "tp"),
        P("sp", "tp", None),
        P("sp", None),
        P(("sp", "tp"), None),
    )
    return jax.shard_map(
        body, mesh=mesh, in_specs=placed, out_specs=P(("sp", "tp"), None), check_vma=False
    )
```

```python
import functools

import jax
import jax.numpy as jnp
from jax import lax
from jax.experimental import pallas as pl
from jax.experimental.pallas import tpu as pltpu
from jax.sharding import PartitionSpec as P

HEAD_DIM = 64
TOPK = 2
GRID_W = 64
TOK_DEV = 256


eps = 1e-06
rope_base = 10000.0


def rotary_tables(positions):
    row_pos = (positions // GRID_W).astype(jnp.float32)
    col_pos = (positions % GRID_W).astype(jnp.float32)
    freq_count = HEAD_DIM // 4
    inverse = rope_base ** (-jnp.arange(freq_count, dtype=jnp.float32) / freq_count)
    angles = jnp.concatenate([row_pos[:, None] * inverse, col_pos[:, None] * inverse], axis=-1)
    return (jnp.cos(angles), jnp.sin(angles))


def prepare(projected, gains, cosine, sine_table):
    tok_total = projected.shape[0]
    head_count = gains.shape[0]
    values_f = projected.astype(jnp.float32).reshape(tok_total, head_count, HEAD_DIM)
    normed = (
        values_f
        * lax.rsqrt(jnp.mean(values_f * values_f, axis=-1, keepdims=True) + eps)
        * gains[None]
    )
    half_dim = HEAD_DIM // 2
    first_half = normed[..., :half_dim]
    second_half = normed[..., half_dim:]
    cos_b = cosine[:, None, :]
    sin_b = sine_table[:, None, :]
    rotated = jnp.concatenate(
        [first_half * cos_b - second_half * sin_b, second_half * cos_b + first_half * sin_b],
        axis=-1,
    )
    return rotated.astype(jnp.bfloat16)


LANES = 128
MESH = pl.DeviceIdType.MESH
LOG2E = 1.4426950408889634


def attention_kernel(
    q_ref, kv_ref, down_ref, out_ref, others_ref,
    qall, kvall, kk, vt, osend, mlsend, orecv, mlrecv, own_o, own_ml, attv,
    qs, qr, ks, kr, os_, or_, ms, mr, xs, xr, ds, dr,
):
    sp = lax.axis_index("sp")
    me_x = lax.axis_index("tp")
    z, j = sp // 8, sp % 8
    tok = q_ref.shape[0]

    def group(d):
        return z * 8 + lax.rem(j + d, 8)

    def ring(d):
        return lax.rem(z + d, 8) * 8 + j

    barrier = pltpu.get_barrier_semaphore()
    for d in range(1, 8):
        pl.semaphore_signal(barrier, inc=1, device_id=(group(d), me_x), device_id_type=MESH)
        pl.semaphore_signal(barrier, inc=1, device_id=(ring(d), me_x), device_id_type=MESH)
    for d in range(1, 4):
        pl.semaphore_signal(barrier, inc=1, device_id=(sp, lax.rem(me_x + d, 4)), device_id_type=MESH)
    pl.semaphore_wait(barrier, 17)

    def q_copy(d):
        return pltpu.make_async_remote_copy(
            src_ref=q_ref, dst_ref=qall.at[d], send_sem=qs.at[d], recv_sem=qr.at[d],
            device_id=(group(d), me_x), device_id_type=MESH)

    def kv_copy(d):
        return pltpu.make_async_remote_copy(
            src_ref=kv_ref, dst_ref=kvall.at[d], send_sem=ks.at[d], recv_sem=kr.at[d],
            device_id=(ring(d), me_x), device_id_type=MESH)

    order = (4, 3, 5, 2, 6, 1, 7)
    for d in order:
        q_copy(d).start()
        kv_copy(d).start()

    right, left = lax.rem(me_x + 1, 4), lax.rem(me_x + 3, 4)
    half = down_ref.shape[0] // 2

    def down_copy(way):
        return pltpu.make_async_remote_copy(
            src_ref=down_ref, dst_ref=others_ref.at[2 * way],
            send_sem=ds.at[way], recv_sem=dr.at[way],
            device_id=(sp, left if way == 0 else right), device_id_type=MESH)

    def down_pass(way):
        part = pl.ds(half * way, half)
        return pltpu.make_async_remote_copy(
            src_ref=others_ref.at[2 * way, part], dst_ref=others_ref.at[1, part],
            send_sem=ds.at[2 + way], recv_sem=dr.at[2 + way],
            device_id=(sp, left if way == 0 else right), device_id_type=MESH)

    for way in range(2):
        down_copy(way).start()

    lane = lax.broadcasted_iota(jnp.int32, (tok, LANES), 1)
    low = lane < HEAD_DIM

    def spread(block, at):
        f = block.astype(jnp.float32)
        kk[pl.ds(at * tok, tok), :] = jnp.where(low, f, pltpu.roll(f, HEAD_DIM, 1)).astype(jnp.bfloat16)
        t = f.T.astype(jnp.bfloat16)
        vt[0:HEAD_DIM, at * tok:(at + 1) * tok] = t[HEAD_DIM:, :]

    vt[HEAD_DIM:, :] = jnp.ones((16, vt.shape[1]), jnp.bfloat16)
    qall[0] = q_ref[...]
    spread(kv_ref[...], 0)
    for d in (1, 7, 2, 6, 3, 5, 4):
        kv_copy(d).wait()
        spread(kvall[d], d)
    for d in range(1, 8):
        q_copy(d).wait()

    chunk = 512
    factor = LOG2E * HEAD_DIM ** (-0.5)

    def o_copy(d):
        return pltpu.make_async_remote_copy(
            src_ref=osend.at[d], dst_ref=orecv.at[d], send_sem=os_.at[d], recv_sem=or_.at[d],
            device_id=(group(8 - d), me_x), device_id_type=MESH)

    def ml_copy(d):
        return pltpu.make_async_remote_copy(
            src_ref=mlsend.at[d], dst_ref=mlrecv.at[d], send_sem=ms.at[d], recv_sem=mr.at[d],
            device_id=(group(8 - d), me_x), device_id_type=MESH)

    def block_of(q):
        zero = jnp.zeros_like(q)
        both = jnp.concatenate([jnp.where(low, q, zero), jnp.where(low, zero, q)], axis=0)
        best = acc = None
        for c in range(8 * tok // chunk):
            keys = kk[c * chunk:(c + 1) * chunk, :]
            s = lax.dot_general(keys, both, (((1,), (1,)), ((), ())), preferred_element_type=jnp.float32)
            top = jnp.max(s, axis=0, keepdims=True)
            new = top if best is None else jnp.maximum(best, top)
            p = jnp.exp2((s - new) * factor).astype(jnp.bfloat16)
            part = jnp.dot(vt[:, c * chunk:(c + 1) * chunk], p, preferred_element_type=jnp.float32)
            acc = part if best is None else acc * jnp.exp2((best - new) * factor) + part
            best = new
        return best, acc

    def put(o_ref, ml_ref, best, acc):
        o_ref[0:HEAD_DIM, :] = acc[0:HEAD_DIM, 0:tok].astype(o_ref.dtype)
        o_ref[HEAD_DIM:, :] = acc[0:HEAD_DIM, tok:].astype(o_ref.dtype)
        ml_ref[0:1, :] = best
        ml_ref[1:2, :] = acc[HEAD_DIM:HEAD_DIM + 1, :]

    def down_turn():
        for way in range(2):
            down_copy(way).wait()
            down_pass(way).start()

    def step(d, carry):
        pl.when(d == 5)(down_turn)
        best, acc = block_of(qall[d])
        put(osend.at[d], mlsend.at[d], best, acc)
        o_copy(d).start()
        ml_copy(d).start()
        return carry

    lax.fori_loop(1, 8, step, 0)
    best, acc = block_of(qall[0])
    put(own_o, own_ml, best, acc)

    def finish(d, carry):
        ml_copy(d).wait()
        o_copy(d).wait()
        return carry

    lax.fori_loop(1, 8, finish, 0)
    tops = [own_ml[0:1, :]] + [mlrecv[d, 0:1, :] for d in range(1, 8)]
    top = functools.reduce(jnp.maximum, tops)
    sums = jnp.zeros_like(top)
    heads = [jnp.zeros((HEAD_DIM, tok), jnp.float32) for _ in range(2)]
    for d in range(8):
        w = jnp.exp2((tops[d] - top) * factor)
        sums = sums + w * (own_ml[1:2, :] if d == 0 else mlrecv[d, 1:2, :])
        o = own_o[...] if d == 0 else orecv[d].astype(jnp.float32)
        for h in range(2):
            heads[h] = heads[h] + o[h * HEAD_DIM:(h + 1) * HEAD_DIM, :] * w[:, h * tok:(h + 1) * tok]
    full = jnp.concatenate([heads[h] / sums[:, h * tok:(h + 1) * tok] for h in range(2)], axis=0)
    rows = full.T.astype(jnp.bfloat16)
    own_rows = tok // 4
    for x in range(4):
        attv[x] = rows[x * own_rows:(x + 1) * own_rows, :]

    def x_copy(d):
        return pltpu.make_async_remote_copy(
            src_ref=attv.at[lax.rem(me_x + d, 4)], dst_ref=out_ref.at[me_x],
            send_sem=xs.at[d], recv_sem=xr.at[d],
            device_id=(sp, lax.rem(me_x + d, 4)), device_id_type=MESH)

    for d in (2, 1, 3):
        x_copy(d).start()
    out_ref[me_x] = attv[me_x]
    for d in (1, 3, 2):
        x_copy(d).wait()
    for way in range(2):
        down_pass(way).wait()


def attention(q, kv, down):
    tok = q.shape[0]
    bf, f32 = jnp.bfloat16, jnp.float32
    dma = pltpu.SemaphoreType.DMA
    return pl.pallas_call(
        attention_kernel,
        out_shape=(jax.ShapeDtypeStruct((4, tok // 4, LANES), bf), jax.ShapeDtypeStruct((3,) + down.shape, bf)),
        in_specs=[pl.BlockSpec(memory_space=pltpu.VMEM)] * 2 + [pl.BlockSpec(memory_space=pl.ANY)],
        out_specs=(pl.BlockSpec(memory_space=pltpu.VMEM), pl.BlockSpec(memory_space=pl.ANY)),
        scratch_shapes=[
            pltpu.VMEM((8, tok, LANES), bf),
            pltpu.VMEM((8, tok, LANES), bf),
            pltpu.VMEM((8 * tok, LANES), bf),
            pltpu.VMEM((HEAD_DIM + 16, 8 * tok), bf),
            pltpu.VMEM((8, LANES, tok), bf),
            pltpu.VMEM((8, 2, 2 * tok), f32),
            pltpu.VMEM((8, LANES, tok), bf),
            pltpu.VMEM((8, 2, 2 * tok), f32),
            pltpu.VMEM((LANES, tok), f32),
            pltpu.VMEM((2, 2 * tok), f32),
            pltpu.VMEM((4, tok // 4, LANES), bf),
        ] + [dma((8,))] * 8 + [dma((4,))] * 4,
        compiler_params=pltpu.CompilerParams(
            collective_id=0, has_side_effects=True, vmem_limit_bytes=48 << 20),
        cost_estimate=pl.CostEstimate(flops=4 * 8 * tok * 8 * tok * 2 * HEAD_DIM, bytes_accessed=1 << 20, transcendentals=0),
    )(q, kv, down)


def order_of(i):
    return lax.rem(8 + (2 * lax.rem(i, 2) - 1) * ((i + 1) // 2), 8)


LAGS = (1, 2, 3)


def expert_kernel(
    src_ref, slot_ref, route_ref, att_ref, resid_ref, outw_ref, gain_ref, gate_ref, up_ref, down_ref, others_ref,
    out_ref,
    dcat, res3, normed3, sendbuf, recv, xall, hall, hsend, retsend, ret, out3,
    dsem, ss, sr, axs, axr, bxs, bxr, hs, hr, ts, tr,
):
    sp = lax.axis_index("sp")
    me_x = lax.axis_index("tp")
    z, j = sp // 8, sp % 8
    right, left = lax.rem(me_x + 1, 4), lax.rem(me_x + 3, 4)

    def peer(k):
        return lax.rem(z + k // 8, 8) * 8 + lax.rem(j + lax.rem(k, 8), 8)

    def source(k):
        return lax.rem(z + 8 - k // 8, 8) * 8 + lax.rem(j + 8 - lax.rem(k, 8), 8)

    own_down = pltpu.make_async_copy(down_ref, dcat.at[0], dsem.at[0])
    other_down = pltpu.make_async_copy(others_ref, dcat.at[pl.ds(1, 3)], dsem.at[1])
    own_down.start()
    other_down.start()
    barrier = pltpu.get_barrier_semaphore()

    def greet(k, carry):
        pl.semaphore_signal(barrier, inc=1, device_id=(peer(k), me_x), device_id_type=MESH)
        return carry

    lax.fori_loop(1, 64, greet, 0)
    for d in range(1, 4):
        pl.semaphore_signal(barrier, inc=1, device_id=(sp, lax.rem(me_x + d, 4)), device_id_type=MESH)

    rows = resid_ref.shape[0]
    mixed = jnp.zeros(resid_ref.shape, jnp.float32)
    for x in range(4):
        mixed = mixed + jnp.dot(att_ref[x], outw_ref[x * LANES:(x + 1) * LANES, :], preferred_element_type=jnp.float32)
    residual = (resid_ref[...].astype(jnp.float32) + mixed).astype(jnp.bfloat16)
    resid_f = residual.astype(jnp.float32)
    scale = lax.rsqrt(jnp.mean(resid_f * resid_f, axis=-1, keepdims=True) + eps)
    normed = (resid_f * scale * gain_ref[...]).astype(jnp.bfloat16)
    res3[...] = residual.reshape(rows, 16, LANES)
    normed3[...] = normed.reshape(rows, 16, LANES)

    def fill(i, carry):
        for k in range(3):
            sendbuf[i, k] = normed3[src_ref[3 * i + k]]
        return carry

    lax.fori_loop(0, 64, fill, 0)
    pl.semaphore_wait(barrier, 66)

    def dispatch(i, carry):
        dz = order_of(i // 8)
        k = dz * 8 + lax.rem(i, 8)

        pltpu.make_async_remote_copy(
            src_ref=sendbuf.at[k], dst_ref=recv.at[dz, lax.rem(i, 8)], send_sem=ss, recv_sem=sr.at[dz],
            device_id=(peer(k), me_x), device_id_type=MESH).start()
        return carry

    lax.fori_loop(1, 64, dispatch, 0)
    recv[0, 0] = sendbuf[0]

    def a_copy(dz, way):
        return pltpu.make_async_remote_copy(
            src_ref=recv.at[dz], dst_ref=xall.at[2 * way, dz],
            send_sem=axs.at[way, dz], recv_sem=axr.at[way, dz],
            device_id=(sp, left if way == 0 else right), device_id_type=MESH)

    def b_copy(dz, way):
        part = pl.ds(4 * way, 4)
        return pltpu.make_async_remote_copy(
            src_ref=xall.at[2 * way, dz, part], dst_ref=xall.at[1, dz, part],
            send_sem=bxs.at[way, dz], recv_sem=bxr.at[way, dz],
            device_id=(sp, left if way == 0 else right), device_id_type=MESH)

    def h_copy(dz, d):
        return pltpu.make_async_remote_copy(
            src_ref=hsend.at[d, dz], dst_ref=hall.at[d, dz],
            send_sem=hs.at[d, dz], recv_sem=hr.at[d, dz],
            device_id=(sp, lax.rem(me_x + d, 4)), device_id_type=MESH)

    def stage_a(dz):
        @pl.when(dz == 0)
        def _():
            pltpu.make_async_copy(recv.at[0, pl.ds(1, 7)], recv.at[0, pl.ds(1, 7)], sr.at[0]).wait()

        @pl.when(dz > 0)
        def _():
            pltpu.make_async_copy(recv.at[dz], recv.at[dz], sr.at[dz]).wait()

        for way in range(2):
            a_copy(dz, way).start()

    def stage_b(dz):
        for way in range(2):
            a_copy(dz, way).wait()
            b_copy(dz, way).start()

    def stage_c(dz):
        for way in range(2):
            b_copy(dz, way).wait()
        block = jnp.concatenate([recv[dz].reshape(24, 16, LANES)] + [xall[d, dz].reshape(24, 16, LANES) for d in range(3)], axis=0)
        block = block.reshape(96, 16 * LANES)
        gate = jnp.dot(block, gate_ref[...], preferred_element_type=jnp.float32)
        upper = jnp.dot(block, up_ref[...], preferred_element_type=jnp.float32)
        hidden = (gate / (1.0 + jnp.exp(-gate)) * upper).astype(jnp.bfloat16)
        hall[0, dz] = hidden[0:24]
        for d in range(1, 4):
            hsend[d, dz] = hidden[24 * d:24 * (d + 1)]
        for d in range(1, 4):
            h_copy(d=d, dz=dz).start()

    def stage_d(dz):
        for d in range(1, 4):
            h_copy(dz, d).wait()
        full = jnp.dot(hall[0, dz], dcat[0], preferred_element_type=jnp.float32)
        for d in range(1, 4):
            full = full + jnp.dot(hall[d, dz], dcat[4 - d], preferred_element_type=jnp.float32)
        tiles = full.astype(jnp.bfloat16).reshape(8, 3, 16, LANES)
        retsend[dz] = tiles

        @pl.when(dz == 0)
        def _():
            ret[0:3] = retsend[0, 0]

        def give(q, carry):
            k = dz * 8 + q
            pltpu.make_async_remote_copy(
                src_ref=retsend.at[dz, q], dst_ref=ret.at[pl.ds(3 * k, 3)], send_sem=ts, recv_sem=tr,
                device_id=(source(k), me_x), device_id_type=MESH).start()
            return carry

        lax.fori_loop(1 - lax.min(dz, 1), 8, give, 0)

    def wait_down():
        own_down.wait()
        other_down.wait()

    la, lb, lc = LAGS

    def step(t, carry):
        pl.when(t < 8)(lambda: stage_a(order_of(t)))
        pl.when((t >= la) & (t < 8 + la))(lambda: stage_b(order_of(t - la)))
        pl.when((t >= lb) & (t < 8 + lb))(lambda: stage_c(order_of(t - lb)))
        pl.when(t == lc)(wait_down)
        pl.when((t >= lc) & (t < 8 + lc))(lambda: stage_d(order_of(t - lc)))
        return carry

    lax.fori_loop(0, 8 + lc, step, 0)
    pltpu.make_async_copy(ret.at[pl.ds(3, 189)], ret.at[pl.ds(3, 189)], tr).wait()

    def join(t, carry):
        total = res3[t].astype(jnp.float32)
        both = jnp.zeros_like(total)
        for k in range(TOPK):
            both = both + ret[slot_ref[TOPK * t + k]].astype(jnp.float32) * route_ref[TOPK * t + k]
        out3[t] = (total + both).astype(jnp.bfloat16)
        return carry

    lax.fori_loop(0, rows, join, 0)
    out_ref[...] = out3[...].reshape(rows, 16 * LANES)
    pltpu.make_async_copy(sendbuf.at[pl.ds(1, 63)], sendbuf.at[pl.ds(1, 63)], ss).wait()
    pltpu.make_async_copy(sendbuf.at[pl.ds(1, 63)], sendbuf.at[pl.ds(1, 63)], ts).wait()


def experts(src, slot, route, att, resid, outw, gain, gate, up, down, others):
    rows = resid.shape[0]
    bf = jnp.bfloat16
    dma = pltpu.SemaphoreType.DMA
    smem = pl.BlockSpec(memory_space=pltpu.SMEM)
    vmem = pl.BlockSpec(memory_space=pltpu.VMEM)
    hbm = pl.BlockSpec(memory_space=pl.ANY)
    return pl.pallas_call(
        expert_kernel,
        out_shape=jax.ShapeDtypeStruct(resid.shape, bf),
        in_specs=[smem] * 3 + [vmem] * 6 + [hbm] * 2,
        out_specs=vmem,
        scratch_shapes=[
            pltpu.VMEM((4,) + down.shape, bf),
            pltpu.VMEM((rows, 16, LANES), bf),
            pltpu.VMEM((rows, 16, LANES), bf),
            pltpu.VMEM((64, 3, 16, LANES), bf),
            pltpu.VMEM((8, 8, 3, 16, LANES), bf),
            pltpu.VMEM((3, 8, 8, 3, 16, LANES), bf),
            pltpu.VMEM((4, 8, 24, down.shape[0]), bf),
            pltpu.VMEM((4, 8, 24, down.shape[0]), bf),
            pltpu.VMEM((8, 8, 3, 16, LANES), bf),
            pltpu.VMEM((192, 16, LANES), bf),
            pltpu.VMEM((rows, 16, LANES), bf),
            dma((2,)), dma(()), dma((8,)), dma((2, 8)), dma((2, 8)), dma((2, 8)), dma((2, 8)),
            dma((4, 8)), dma((4, 8)), dma(()), dma(()),
        ],
        compiler_params=pltpu.CompilerParams(
            collective_id=1, has_side_effects=True, vmem_limit_bytes=56 << 20),
        cost_estimate=pl.CostEstimate(flops=6 * 768 * 2048 * 256, bytes_accessed=8 << 20, transcendentals=0),
    )(src, slot, route, att, resid, outw, gain, gate, up, down, others)


def routing(own_ids):
    sp = lax.axis_index("sp")
    flat = own_ids.reshape(-1)
    count = flat.shape[0]
    item = jnp.arange(count, dtype=jnp.int32)
    earlier = (flat[:, None] == flat[None, :]) & (item[None, :] < item[:, None])
    rank = jnp.sum(earlier.astype(jnp.int32), axis=1)
    place = ((flat // 8 - sp // 8) % 8) * 8 + (flat - sp) % 8
    slot = place * 3 + rank
    named = jnp.arange(192, dtype=jnp.int32)[:, None] == slot[None, :]
    src = jnp.sum(jnp.where(named, item[None, :] // TOPK, 0), axis=1)
    return slot, src


def body(
    resid_in,
    query_proj,
    key_proj,
    value_proj,
    query_gain,
    key_gain,
    out_weight,
    norm_gain,
    gate_weight,
    up_weight,
    down_weight,
    expert_ids,
    route_weight,
):
    tok_count = query_proj.shape[0]
    head_local = query_gain.shape[0]
    positions = lax.axis_index("sp") * tok_count + lax.iota(jnp.int32, tok_count)
    cosine, sine_table = rotary_tables(positions)
    query_rot = prepare(query_proj, query_gain, cosine, sine_table)
    key_rot = prepare(key_proj, key_gain, cosine, sine_table)
    row_count = tok_count // lax.axis_size("tp")
    own_ids = lax.dynamic_slice_in_dim(expert_ids, lax.axis_index("tp") * row_count, row_count, 0)
    slot, src = routing(own_ids)
    regrouped, others = attention(
        query_rot.reshape(tok_count, head_local * HEAD_DIM),
        jnp.concatenate([key_rot.reshape(tok_count, HEAD_DIM), value_proj], axis=1),
        down_weight[0],
    )
    return experts(
        src, slot, route_weight.reshape(-1), regrouped, resid_in, out_weight, norm_gain[None],
        gate_weight[0], up_weight[0], down_weight[0], others,
    )


def solution(mesh):
    placed = (
        P(("sp", "tp"), None),
        P("sp", "tp"),
        P("sp", "tp"),
        P("sp", "tp"),
        P("tp", None),
        P("tp", None),
        P(),
        P(),
        P("sp", None, "tp"),
        P("sp", None, "tp"),
        P("sp", "tp", None),
        P("sp", None),
        P(("sp", "tp"), None),
    )
    return jax.shard_map(
        body, mesh=mesh, in_specs=placed, out_specs=P(("sp", "tp"), None), check_vma=False
    )
```

```python
import functools
import math

import jax
import jax.numpy as jnp
from jax import lax
from jax.experimental import pallas as pl
from jax.experimental.pallas import tpu as pltpu
from jax.sharding import PartitionSpec as P

HEAD_DIM = 64
TOPK = 2
GRID_W = 64
TOK_DEV = 256

eps = 1e-06
rope_base = 10000.0

LANES = 128
MESH = pl.DeviceIdType.MESH
NEAR = (0, 1, 7, 2, 6, 3, 5, 4)
GROUPS = (0, 2, 4, 5, 3, 6, 1, 7)
CHUNK = 512


def near_first(i):
    return lax.rem(8 + (2 * lax.rem(i, 2) - 1) * ((i + 1) // 2), 8)


def rotary_tables(sp):
    shape = (GRID_W + 8, LANES)
    freq_count = HEAD_DIM // 4
    lane = lax.broadcasted_iota(jnp.int32, shape, 1)
    item = lax.broadcasted_iota(jnp.int32, shape, 0)
    position = jnp.where(item < GRID_W, item, item - GRID_W + sp * (TOK_DEV // GRID_W)).astype(jnp.float32)
    index = lax.rem(lane, freq_count).astype(jnp.float32)
    angles = position * jnp.exp(index * (-math.log(rope_base) / freq_count))
    row_lane = lax.rem(lane[:GRID_W], 2 * freq_count) < freq_count

    def table(values):
        col = values[:GRID_W]
        return jnp.concatenate(
            [jnp.where(row_lane, values[GRID_W + r:GRID_W + r + 1], col) for r in range(TOK_DEV // GRID_W)], axis=0)

    return table(jnp.cos(angles)), table(jnp.sin(angles))


def prepare(values_f, gains, cosine, sine_table):
    lane = lax.broadcasted_iota(jnp.int32, values_f.shape, 1)
    low = lane < HEAD_DIM
    squares = values_f * values_f
    first = jnp.sum(jnp.where(low, squares, 0.0), axis=-1, keepdims=True)
    second = jnp.sum(jnp.where(low, 0.0, squares), axis=-1, keepdims=True)
    scale = jnp.where(low, lax.rsqrt(first / HEAD_DIM + eps), lax.rsqrt(second / HEAD_DIM + eps))
    normed = values_f * scale * gains
    half_dim = HEAD_DIM // 2
    turned = jnp.where(
        lax.rem(lane, HEAD_DIM) < half_dim, -pltpu.roll(normed, LANES - half_dim, 1), pltpu.roll(normed, half_dim, 1))
    return normed * cosine + turned * sine_table


def layer_kernel(
    src_ref, slot_ref, route_ref, query_ref, key_ref, value_ref, qgain_ref, kgain_ref, resid_ref, gain_ref,
    outw_hbm, gate_hbm, up_hbm, down_hbm,
    out_ref,
    qall, kvall, kk, vt, best_s, acc_s, osend, mlsend, orecv, mlrecv, attv, att,
    outw, gatew, upw, dcat, res3, normed3, sendbuf, recv, xall, hall, hsend, retsend, ret, out3,
    wsem, qs, qr, ks, kr, ps, pr, ms, mr, xs, xr, ds, dr,
    ss, sr, axs, axr, bxs, bxr, hs, hr, ts, tr,
):
    sp = lax.axis_index("sp")
    me_x = lax.axis_index("tp")
    z, j = sp // 8, lax.rem(sp, 8)
    right, left = lax.rem(me_x + 1, 4), lax.rem(me_x + 3, 4)
    tok = query_ref.shape[0]
    rows = resid_ref.shape[0]
    bf, f32 = jnp.bfloat16, jnp.float32

    def at_offset(dz, dj):
        return lax.rem(z + dz, 8) * 8 + lax.rem(j + dj, 8)

    def remote(src, dst, send, recv_sem, sp_to, x_to):
        return pltpu.make_async_remote_copy(
            src_ref=src, dst_ref=dst, send_sem=send, recv_sem=recv_sem,
            device_id=(sp_to, x_to), device_id_type=MESH)

    barrier = pltpu.get_barrier_semaphore()

    with jax.named_scope("greet"):
        for d in range(1, 4):
            pl.semaphore_signal(barrier, inc=1, device_id=(sp, lax.rem(me_x + d, 4)), device_id_type=MESH)
        for d in range(1, 8):
            for dz, dj in ((0, d), (d, 0)):
                pl.semaphore_signal(barrier, inc=1, device_id=(at_offset(dz, dj), me_x), device_id_type=MESH)

    weights = [
        pltpu.make_async_copy(a, b, wsem.at[n])
        for n, (a, b) in enumerate(((outw_hbm, outw), (gate_hbm, gatew), (up_hbm, upw), (down_hbm, dcat.at[0])))
    ]
    for copy in weights:
        copy.start()

    with jax.named_scope("prep"):
        lane = lax.broadcasted_iota(jnp.int32, (tok, LANES), 1)
        low = lane < HEAD_DIM
        cosine, sine_table = rotary_tables(sp)
        qgain = jnp.concatenate([qgain_ref[0:1, :], qgain_ref[1:2, :]], axis=1)
        qall[0] = prepare(query_ref[...].astype(f32), qgain, cosine, sine_table).astype(bf)
        key_value = jnp.concatenate([key_ref[...].astype(f32), value_ref[...].astype(f32)], axis=0).T
        kgain = jnp.concatenate([kgain_ref[...], kgain_ref[...]], axis=1)
        kvall[0] = jnp.where(low, prepare(key_value, kgain, cosine, sine_table), key_value).astype(bf)
        vt[HEAD_DIM:, :] = jnp.ones((16, vt.shape[1]), bf)
        best_s[...] = jnp.full(best_s.shape, -1e30, f32)
        acc_s[...] = jnp.zeros(acc_s.shape, f32)
    with jax.named_scope("barrier"):
        pl.semaphore_wait(barrier, 17)

    def q_copy(d):
        return remote(qall.at[0], qall.at[d], qs.at[d], qr.at[d], at_offset(0, d), me_x)

    def kv_copy(d):
        return remote(kvall.at[0], kvall.at[d], ks.at[d], kr.at[d], at_offset(d, 0), me_x)

    half = down_hbm.shape[0] // 2
    quarter = half // 2

    def down_copy(way):
        return remote(down_hbm, dcat.at[1 + 2 * way], ds.at[way], dr.at[way], sp, left if way == 0 else right)

    def down_pass(way, n):
        part = pl.ds(half * way + quarter * n, quarter)
        return remote(
            dcat.at[1 + 2 * way, part], dcat.at[2, part], ds.at[2 + 2 * n + way], dr.at[2 + 2 * n + way],
            sp, left if way == 0 else right)

    with jax.named_scope("issue"):
        for d in NEAR[1:]:
            kv_copy(d).start()
            q_copy(d).start()
        for way in range(2):
            down_copy(way).start()

    def spread(n):
        f = kvall[NEAR[n]].astype(f32)
        kk[n * tok:(n + 1) * tok, :] = jnp.where(low, f, pltpu.roll(f, HEAD_DIM, 1)).astype(bf)
        vt[0:HEAD_DIM, n * tok:(n + 1) * tok] = f.T[HEAD_DIM:, :].astype(bf)

    with jax.named_scope("spread1"):
        spread(0)
        for n in range(1, 4):
            with jax.named_scope(f"wait_kv{n}"):
                kv_copy(NEAR[n]).wait()
            spread(n)

    factor = math.log2(math.e) * HEAD_DIM ** (-0.5)

    def o_copy(d):
        return remote(osend.at[d], orecv.at[d], ps.at[d], pr.at[d], at_offset(0, 8 - d), me_x)

    def ml_copy(d):
        return remote(mlsend.at[d], mlrecv.at[d], ms.at[d], mr.at[d], at_offset(0, 8 - d), me_x)

    def second_half():
        for n in range(4, 8):
            with jax.named_scope(f"wait_kv{n}"):
                kv_copy(NEAR[n]).wait()
            spread(n)

    def down_turn():
        for way in range(2):
            down_copy(way).wait()
            down_pass(way, 0).start()

    def attend(i, carry):
        part = i // 8
        turn = lax.rem(i, 8)
        d = near_first(turn + part * (7 - 2 * turn))
        with jax.named_scope("wait_q"):
            pl.when((part == 0) & (d > 0))(lambda: q_copy(d).wait())
        pl.when(i == 8)(second_half)
        with jax.named_scope("down_turn"):
            pl.when(i == 14)(down_turn)
        with jax.named_scope("attend"):
            q = qall[d]
            zero = jnp.zeros_like(q)
            both = jnp.concatenate([jnp.where(low, q, zero), jnp.where(low, zero, q)], axis=0)
            best = best_s[d]
            acc = acc_s[d]
            for c in range(4 * tok // CHUNK):
                begin = pl.multiple_of(part * (4 * tok) + c * CHUNK, CHUNK)
                s = lax.dot_general(
                    kk[pl.ds(begin, CHUNK), :], both, (((1,), (1,)), ((), ())), preferred_element_type=f32)
                new = jnp.maximum(best, jnp.max(s, axis=0, keepdims=True))
                p = jnp.exp2((s - new) * factor).astype(bf)
                acc = acc * jnp.exp2((best - new) * factor) + jnp.dot(
                    vt[:, pl.ds(begin, CHUNK)], p, preferred_element_type=f32)
                best = new
            best_s[d] = best
            acc_s[d] = acc

        @pl.when(part == 1)
        def _():
            osend[d, 0:HEAD_DIM, :] = acc[0:HEAD_DIM, 0:tok].astype(bf)
            osend[d, HEAD_DIM:, :] = acc[0:HEAD_DIM, tok:].astype(bf)
            mlsend[d, 0:1, :] = best
            mlsend[d, 1:2, :] = acc[HEAD_DIM:HEAD_DIM + 1, :]

        @pl.when((part == 1) & (d > 0))
        def _():
            o_copy(d).start()
            ml_copy(d).start()

        return carry

    lax.fori_loop(0, 16, attend, 0)

    def finish(d, carry):
        ml_copy(d).wait()
        o_copy(d).wait()
        return carry

    with jax.named_scope("wait_part"):
        lax.fori_loop(1, 8, finish, 0)
    with jax.named_scope("combine"):
        tops = [mlsend[0, 0:1, :]] + [mlrecv[d, 0:1, :] for d in range(1, 8)]
        top = functools.reduce(jnp.maximum, tops)
        sums = jnp.zeros_like(top)
        heads = [jnp.zeros((HEAD_DIM, tok), f32) for _ in range(2)]
        for d in range(8):
            w = jnp.exp2((tops[d] - top) * factor)
            sums = sums + w * (mlsend[0, 1:2, :] if d == 0 else mlrecv[d, 1:2, :])
            o = (osend[0] if d == 0 else orecv[d]).astype(f32)
            for h in range(2):
                heads[h] = heads[h] + o[h * HEAD_DIM:(h + 1) * HEAD_DIM, :] * w[:, h * tok:(h + 1) * tok]
        full = jnp.concatenate([heads[h] / sums[:, h * tok:(h + 1) * tok] for h in range(2)], axis=0)
        joined = full.T.astype(bf)
        for x in range(4):
            attv[x] = joined[x * rows:(x + 1) * rows, :]

    def x_copy(d):
        to = lax.rem(me_x + d, 4)
        return remote(attv.at[to], att.at[me_x], xs.at[d], xr.at[d], sp, to)

    with jax.named_scope("x_exchange"):
        for d in (2, 1, 3):
            x_copy(d).start()
        att[me_x] = attv[me_x]
        weights[0].wait()
        for d in (1, 3, 2):
            x_copy(d).wait()
    for way in range(2):
        down_pass(way, 1).start()

    with jax.named_scope("proj"):
        mixed = jnp.zeros(resid_ref.shape, f32)
        for x in range(4):
            mixed = mixed + jnp.dot(att[x], outw[x * LANES:(x + 1) * LANES, :], preferred_element_type=f32)
        residual = (resid_ref[...].astype(f32) + mixed).astype(bf)
        resid_f = residual.astype(f32)
        scale = lax.rsqrt(jnp.mean(resid_f * resid_f, axis=-1, keepdims=True) + eps)
        normed = (resid_f * scale * gain_ref[...]).astype(bf)
        res3[...] = residual.reshape(rows, 16, LANES)
        normed3[...] = normed.reshape(rows, 16, LANES)

    def fill(i, carry):
        for k in range(3):
            sendbuf[i, k] = normed3[src_ref[3 * i + k]]
        return carry

    with jax.named_scope("fill"):
        lax.fori_loop(0, 64, fill, 0)

    with jax.named_scope("dispatch"):
        for dz in GROUPS:
            def dispatch(dj, carry, dz=dz):
                remote(sendbuf.at[dz * 8 + dj], recv.at[dz, dj], ss, sr.at[dz], at_offset(dz, dj), me_x).start()
                return carry

            lax.fori_loop(1 if dz == 0 else 0, 8, dispatch, 0)
        recv[0, 0] = sendbuf[0]

    def a_copy(dz, way):
        return remote(
            recv.at[dz], xall.at[2 * way, dz], axs.at[way, dz], axr.at[way, dz], sp, left if way == 0 else right)

    def b_copy(dz, way):
        part = pl.ds(4 * way, 4)
        return remote(
            xall.at[2 * way, dz, part], xall.at[1, dz, part], bxs.at[way, dz], bxr.at[way, dz],
            sp, left if way == 0 else right)

    def h_copy(dz, d):
        return remote(hsend.at[d, dz], hall.at[d, dz], hs.at[d, dz], hr.at[d, dz], sp, lax.rem(me_x + d, 4))

    def stage_a(dz):
        with jax.named_scope(f"A{dz}"):
            arrived = recv.at[0, pl.ds(1, 7)] if dz == 0 else recv.at[dz]
            pltpu.make_async_copy(arrived, arrived, sr.at[dz]).wait()
            for way in range(2):
                a_copy(dz, way).start()

    def stage_b(dz):
        with jax.named_scope(f"B{dz}"):
            for way in range(2):
                a_copy(dz, way).wait()
                b_copy(dz, way).start()

    def stage_c(pair):
        with jax.named_scope(f"Cw{pair[0]}"):
            for dz in pair:
                for way in range(2):
                    b_copy(dz, way).wait()
        with jax.named_scope(f"C{pair[0]}"):
            block = jnp.concatenate(
                [recv[dz].reshape(24, 16, LANES) for dz in pair]
                + [xall[d, dz].reshape(24, 16, LANES) for d in range(3) for dz in pair], axis=0)
            block = block.reshape(block.shape[0], 16 * LANES)
            gate = jnp.dot(block, gatew[...], preferred_element_type=f32)
            upper = jnp.dot(block, upw[...], preferred_element_type=f32)
            hidden = (gate / (1.0 + jnp.exp(-gate)) * upper).astype(bf)
            for n, dz in enumerate(pair):
                hall[0, dz] = hidden[24 * n:24 * (n + 1)]
                for d in range(1, 4):
                    begin = 24 * (len(pair) * d + n)
                    hsend[d, dz] = hidden[begin:begin + 24]
            for dz in pair:
                for d in range(1, 4):
                    h_copy(dz, d).start()

    def stage_d(pair):
        with jax.named_scope(f"Dw{pair[0]}"):
            for dz in pair:
                for d in range(1, 4):
                    h_copy(dz, d).wait()
        with jax.named_scope(f"D{pair[0]}"):
            full = None
            for d in range(4):
                hidden = jnp.concatenate([hall[d, dz] for dz in pair], axis=0)
                term = jnp.dot(hidden, dcat[(4 - d) % 4], preferred_element_type=f32)
                full = term if full is None else full + term
            tiles = full.astype(bf).reshape(len(pair), 8, 3, 16, LANES)
            for n, dz in enumerate(pair):
                retsend[dz] = tiles[n]
            for dz in pair:
                def give(dj, carry, dz=dz):
                    remote(
                        retsend.at[dz, dj], ret.at[pl.ds(24 * dz + 3 * dj, 3)], ts, tr,
                        at_offset(8 - dz, 8 - dj), me_x).start()
                    return carry

                if dz == 0:
                    ret[0:3] = retsend[0, 0]
                lax.fori_loop(1 if dz == 0 else 0, 8, give, 0)

    pairs = [GROUPS[n:n + 2] for n in range(0, 8, 2)]

    def both_of(stage, n):
        for dz in pairs[n]:
            stage(dz)

    def wait_down():
        with jax.named_scope("wait_down"):
            weights[3].wait()
            for way in range(2):
                for n in range(2):
                    down_pass(way, n).wait()

    both_of(stage_a, 0)
    both_of(stage_b, 0)
    both_of(stage_a, 1)
    weights[1].wait()
    weights[2].wait()
    stage_c(pairs[0])
    both_of(stage_b, 1)
    both_of(stage_a, 2)
    wait_down()
    stage_d(pairs[0])
    stage_c(pairs[1])
    both_of(stage_b, 2)
    both_of(stage_a, 3)
    stage_d(pairs[1])
    stage_c(pairs[2])
    both_of(stage_b, 3)
    stage_d(pairs[2])
    stage_c(pairs[3])
    stage_d(pairs[3])

    with jax.named_scope("wait_ret"):
        pltpu.make_async_copy(ret.at[pl.ds(3, 189)], ret.at[pl.ds(3, 189)], tr).wait()

    def join(t, carry):
        both = jnp.zeros((16, LANES), f32)
        for k in range(TOPK):
            both = both + ret[slot_ref[TOPK * t + k]].astype(f32) * route_ref[k, t]
        out3[t] = (res3[t].astype(f32) + both).astype(bf)
        return carry

    with jax.named_scope("join"):
        lax.fori_loop(0, rows, join, 0)
        out_ref[...] = out3[...].reshape(rows, 16 * LANES)
    pltpu.make_async_copy(sendbuf.at[pl.ds(1, 63)], sendbuf.at[pl.ds(1, 63)], ss).wait()
    pltpu.make_async_copy(sendbuf.at[pl.ds(1, 63)], sendbuf.at[pl.ds(1, 63)], ts).wait()


def routing(own_ids):
    sp = lax.axis_index("sp")
    flat = own_ids.reshape(-1)
    count = flat.shape[0]
    item = jnp.arange(count, dtype=jnp.int32)
    earlier = (flat[:, None] == flat[None, :]) & (item[None, :] < item[:, None])
    rank = jnp.sum(earlier.astype(jnp.int32), axis=1)
    place = ((flat // 8 - sp // 8) % 8) * 8 + (flat - sp) % 8
    slot = place * 3 + rank
    named = jnp.arange(192, dtype=jnp.int32)[:, None] == slot[None, :]
    src = jnp.sum(jnp.where(named, item[None, :] // TOPK, 0), axis=1)
    return slot, src


def body(
    resid_in,
    query_proj,
    key_proj,
    value_proj,
    query_gain,
    key_gain,
    out_weight,
    norm_gain,
    gate_weight,
    up_weight,
    down_weight,
    expert_ids,
    route_weight,
):
    tok = query_proj.shape[0]
    rows = resid_in.shape[0]
    own_ids = lax.dynamic_slice_in_dim(expert_ids, lax.axis_index("tp") * rows, rows, 0)
    slot, src = routing(own_ids)
    ff = down_weight.shape[1]
    bf, f32 = jnp.bfloat16, jnp.float32
    dma = pltpu.SemaphoreType.DMA
    smem = pl.BlockSpec(memory_space=pltpu.SMEM)
    vmem = pl.BlockSpec(memory_space=pltpu.VMEM)
    hbm = pl.BlockSpec(memory_space=pl.ANY)
    return pl.pallas_call(
        layer_kernel,
        out_shape=jax.ShapeDtypeStruct(resid_in.shape, bf),
        in_specs=[smem] * 3 + [vmem] * 7 + [hbm] * 4,
        out_specs=vmem,
        scratch_shapes=[
            pltpu.VMEM((8, tok, LANES), bf),
            pltpu.VMEM((8, tok, LANES), bf),
            pltpu.VMEM((8 * tok, LANES), bf),
            pltpu.VMEM((HEAD_DIM + 16, 8 * tok), bf),
            pltpu.VMEM((8, 1, 2 * tok), f32),
            pltpu.VMEM((8, HEAD_DIM + 16, 2 * tok), f32),
            pltpu.VMEM((8, LANES, tok), bf),
            pltpu.VMEM((8, 2, 2 * tok), f32),
            pltpu.VMEM((8, LANES, tok), bf),
            pltpu.VMEM((8, 2, 2 * tok), f32),
            pltpu.VMEM((4, rows, LANES), bf),
            pltpu.VMEM((4, rows, LANES), bf),
            pltpu.VMEM(out_weight.shape, bf),
            pltpu.VMEM(gate_weight.shape[1:], bf),
            pltpu.VMEM(up_weight.shape[1:], bf),
            pltpu.VMEM((4,) + down_weight.shape[1:], bf),
            pltpu.VMEM((rows, 16, LANES), bf),
            pltpu.VMEM((rows, 16, LANES), bf),
            pltpu.VMEM((64, 3, 16, LANES), bf),
            pltpu.VMEM((8, 8, 3, 16, LANES), bf),
            pltpu.VMEM((3, 8, 8, 3, 16, LANES), bf),
            pltpu.VMEM((4, 8, 24, ff), bf),
            pltpu.VMEM((4, 8, 24, ff), bf),
            pltpu.VMEM((8, 8, 3, 16, LANES), bf),
            pltpu.VMEM((192, 16, LANES), bf),
            pltpu.VMEM((rows, 16, LANES), bf),
        ] + [dma((4,))] + [dma((8,))] * 8 + [dma((4,))] * 2 + [dma((6,))] * 2
        + [dma(()), dma((8,))] + [dma((2, 8))] * 4 + [dma((4, 8))] * 2 + [dma(())] * 2,
        compiler_params=pltpu.CompilerParams(
            collective_id=0, has_side_effects=True, vmem_limit_bytes=60 << 20),
    )(
        src, slot, route_weight.T, query_proj, key_proj.T, value_proj.T, query_gain, key_gain, resid_in,
        norm_gain[None], out_weight, gate_weight[0], up_weight[0], down_weight[0],
    )


def solution(mesh):
    placed = (
        P(("sp", "tp"), None),
        P("sp", "tp"),
        P("sp", "tp"),
        P("sp", "tp"),
        P("tp", None),
        P("tp", None),
        P(),
        P(),
        P("sp", None, "tp"),
        P("sp", None, "tp"),
        P("sp", "tp", None),
        P("sp", None),
        P(("sp", "tp"), None),
    )
    return jax.shard_map(
        body, mesh=mesh, in_specs=placed, out_specs=P(("sp", "tp"), None), check_vma=False
    )
```

```python
import functools
import math

import jax
import jax.numpy as jnp
from jax import lax
from jax.experimental import pallas as pl
from jax.experimental.pallas import tpu as pltpu
from jax.sharding import PartitionSpec as P

HEAD_DIM = 64
TOPK = 2
GRID_W = 64
TOK_DEV = 256

eps = 1e-06
rope_base = 10000.0

LANES = 128
MESH = pl.DeviceIdType.MESH
NEAR = (0, 1, 7, 2, 6, 3, 5, 4)
LEAD = 3
GROUPS = (0, 1, 4, 5, 3, 6, 2, 7)
PARTS = (((0, 512), (512, 256)), ((768, 512),), ((1280, 512), (1792, 256)))


def near_first(i):
    return lax.rem(8 + (2 * lax.rem(i, 2) - 1) * ((i + 1) // 2), 8)


def rotary_tables(sp):
    shape = (GRID_W + 8, LANES)
    freq_count = HEAD_DIM // 4
    lane = lax.broadcasted_iota(jnp.int32, shape, 1)
    item = lax.broadcasted_iota(jnp.int32, shape, 0)
    position = jnp.where(item < GRID_W, item, item - GRID_W + sp * (TOK_DEV // GRID_W)).astype(jnp.float32)
    index = lax.rem(lane, freq_count).astype(jnp.float32)
    angles = position * jnp.exp(index * (-math.log(rope_base) / freq_count))
    row_lane = lax.rem(lane[:GRID_W], 2 * freq_count) < freq_count

    def table(values):
        col = values[:GRID_W]
        return jnp.concatenate(
            [jnp.where(row_lane, values[GRID_W + r:GRID_W + r + 1], col) for r in range(TOK_DEV // GRID_W)], axis=0)

    return table(jnp.cos(angles)), table(jnp.sin(angles))


def prepare(values_f, gains, cosine, sine_table):
    lane = lax.broadcasted_iota(jnp.int32, values_f.shape, 1)
    low = lane < HEAD_DIM
    squares = values_f * values_f
    first = jnp.sum(jnp.where(low, squares, 0.0), axis=-1, keepdims=True)
    second = jnp.sum(jnp.where(low, 0.0, squares), axis=-1, keepdims=True)
    scale = jnp.where(low, lax.rsqrt(first / HEAD_DIM + eps), lax.rsqrt(second / HEAD_DIM + eps))
    normed = values_f * scale * gains
    half_dim = HEAD_DIM // 2
    turned = jnp.where(
        lax.rem(lane, HEAD_DIM) < half_dim, -pltpu.roll(normed, LANES - half_dim, 1), pltpu.roll(normed, half_dim, 1))
    return normed * cosine + turned * sine_table


def layer_kernel(
    ids_ref, route_ref, query_ref, key_ref, value_ref, qgain_ref, kgain_ref, resid_ref, gain_ref,
    outw_hbm, gate_hbm, up_hbm, down_hbm,
    out_ref,
    qall, kvall, kk, vt, best_s, acc_s, osend, mlsend, orecv, mlrecv, attv, att,
    outw, gatew, upw, dcat, pick, joiner, resid_s, sendbuf, recv, xall, hall, hsend, retsend, ret,
    wsem, qs, qr, ks, kr, ps, pr, ms, mr, xs, xr, ds, dr,
    ss, sr, axs, axr, bxs, bxr, hs, hr, ts, tr,
):
    sp = lax.axis_index("sp")
    me_x = lax.axis_index("tp")
    z, j = sp // 8, lax.rem(sp, 8)
    right, left = lax.rem(me_x + 1, 4), lax.rem(me_x + 3, 4)
    tok = query_ref.shape[0]
    rows = resid_ref.shape[0]
    bf, f32 = jnp.bfloat16, jnp.float32

    def at_offset(dz, dj):
        return lax.rem(z + dz, 8) * 8 + lax.rem(j + dj, 8)

    def remote(src, dst, send, recv_sem, sp_to, x_to):
        return pltpu.make_async_remote_copy(
            src_ref=src, dst_ref=dst, send_sem=send, recv_sem=recv_sem,
            device_id=(sp_to, x_to), device_id_type=MESH)

    barrier = pltpu.get_barrier_semaphore()

    with jax.named_scope("greet"):
        for d in range(1, 4):
            pl.semaphore_signal(barrier, inc=1, device_id=(sp, lax.rem(me_x + d, 4)), device_id_type=MESH)
        for d in range(1, 8):
            for dz, dj in ((0, d), (d, 0)):
                pl.semaphore_signal(barrier, inc=1, device_id=(at_offset(dz, dj), me_x), device_id_type=MESH)

    weights = [
        pltpu.make_async_copy(a, b, wsem.at[n])
        for n, (a, b) in enumerate(((outw_hbm, outw), (gate_hbm, gatew), (up_hbm, upw), (down_hbm, dcat.at[0])))
    ]
    for copy in weights:
        copy.start()

    with jax.named_scope("prep"):
        lane = lax.broadcasted_iota(jnp.int32, (tok, LANES), 1)
        low = lane < HEAD_DIM
        cosine, sine_table = rotary_tables(sp)
        qgain = jnp.concatenate([qgain_ref[0:1, :], qgain_ref[1:2, :]], axis=1)
        qall[0] = prepare(query_ref[...].astype(f32), qgain, cosine, sine_table).astype(bf)
        key_value = jnp.concatenate([key_ref[...].astype(f32), value_ref[...].astype(f32)], axis=0).T
        kgain = jnp.concatenate([kgain_ref[...], kgain_ref[...]], axis=1)
        kvall[0] = jnp.where(low, prepare(key_value, kgain, cosine, sine_table), key_value).astype(bf)
        vt[HEAD_DIM:, :] = jnp.ones((16, vt.shape[1]), bf)
    with jax.named_scope("barrier"):
        pl.semaphore_wait(barrier, 17)

    def q_copy(d):
        return remote(qall.at[0], qall.at[d], qs.at[d], qr.at[d], at_offset(0, d), me_x)

    def kv_copy(d):
        return remote(kvall.at[0], kvall.at[d], ks.at[d], kr.at[d], at_offset(d, 0), me_x)

    half = down_hbm.shape[0] // 2
    quarter = half // 4

    def down_copy(way):
        return remote(down_hbm, dcat.at[1 + 2 * way], ds.at[way], dr.at[way], sp, left if way == 0 else right)

    def down_pass(way, n):
        part = pl.ds(half * way + quarter * n, quarter)
        return remote(
            dcat.at[1 + 2 * way, part], dcat.at[2, part], ds.at[2 + 2 * n + way], dr.at[2 + 2 * n + way],
            sp, left if way == 0 else right)

    with jax.named_scope("issue"):
        for d in NEAR[1:3]:
            kv_copy(d).start()
        for d in NEAR[1:]:
            q_copy(d).start()
        for d in NEAR[3:]:
            kv_copy(d).start()
        for way in range(2):
            down_copy(way).start()

    def spread(n):
        f = kvall[NEAR[n]].astype(f32)
        kk[n * tok:(n + 1) * tok, :] = jnp.where(low, f, pltpu.roll(f, HEAD_DIM, 1)).astype(bf)
        vt[0:HEAD_DIM, n * tok:(n + 1) * tok] = f.T[HEAD_DIM:, :].astype(bf)

    with jax.named_scope("routing"):
        ids = ids_ref[0:2, 0:rows]
        for x in range(1, 4):
            ids = jnp.where(me_x == x, ids_ref[0:2, x * rows:(x + 1) * rows], ids)
        ids = ids.astype(f32)
        items = TOPK * rows
        flat = jnp.broadcast_to(jnp.concatenate([ids[0:1], ids[1:2]], axis=1), (items, items))
        turned = flat.T
        same = flat == turned
        first = lax.broadcasted_iota(jnp.int32, (items, items), 0)
        second = lax.broadcasted_iota(jnp.int32, (items, items), 1)

        def slot_of(e, rank):
            e = e.astype(jnp.int32)
            place = lax.rem(lax.div(e, 8) + 8 - z, 8) * 8 + lax.rem(lax.rem(e, 8) + 8 - j, 8)
            return place * 3 + rank.astype(jnp.int32)

        across = slot_of(flat[0:1], jnp.sum(jnp.where(same & (first < second), 1.0, 0.0), axis=0, keepdims=True))
        down = slot_of(turned[:, 0:1], jnp.sum(jnp.where(same & (second < first), 1.0, 0.0), axis=1, keepdims=True))
        pick[...] = jnp.where(lax.broadcasted_iota(jnp.int32, pick.shape, 0) == across, 1.0, 0.0).astype(bf)
        joiner[...] = jnp.where(lax.broadcasted_iota(jnp.int32, joiner.shape, 1) == down, 1.0, 0.0).astype(bf)

    with jax.named_scope("spread1"):
        spread(0)
        for n in range(1, 3):
            with jax.named_scope(f"wait_kv{n}"):
                kv_copy(NEAR[n]).wait()
            spread(n)

    factor = math.log2(math.e) * HEAD_DIM ** (-0.5)

    def o_copy(d):
        return remote(osend.at[d], orecv.at[d], ps.at[d], pr.at[d], at_offset(0, 8 - d), me_x)

    def ml_copy(d):
        return remote(mlsend.at[d], mlrecv.at[d], ms.at[d], mr.at[d], at_offset(0, 8 - d), me_x)

    def pass_on(n):
        for way in range(2):
            down_pass(way, n).start()

    def attend(d, spans, best, acc):
        with jax.named_scope("attend"):
            q = qall[d]
            zero = jnp.zeros_like(q)
            both = jnp.concatenate([jnp.where(low, q, zero), jnp.where(low, zero, q)], axis=0)

            def scores(span):
                return lax.dot_general(
                    kk[span[0]:span[0] + span[1], :], both, (((1,), (1,)), ((), ())), preferred_element_type=f32)

            s = scores(spans[0])
            for n, (begin, size) in enumerate(spans):
                ahead = scores(spans[n + 1]) if n + 1 < len(spans) else None
                new = jnp.max(s, axis=0, keepdims=True)
                if best is not None:
                    new = jnp.maximum(best, new)
                p = jnp.exp2((s - new) * factor).astype(bf)
                part = jnp.dot(vt[:, begin:begin + size], p, preferred_element_type=f32)
                acc = part if best is None else acc * jnp.exp2((best - new) * factor) + part
                best, s = new, ahead
            return best, acc

    def early(i, carry):
        d = near_first(i)
        with jax.named_scope("wait_q"):
            pl.when(d > 0)(lambda: q_copy(d).wait())
        best, acc = attend(d, PARTS[0], None, None)
        best_s[d] = best
        acc_s[d] = acc
        return carry

    def middle(d, carry):
        best, acc = attend(d, PARTS[1], best_s[d], acc_s[d])
        best_s[d] = best
        acc_s[d] = acc
        return carry

    lax.fori_loop(0, 8, early, 0)
    with jax.named_scope("spread2"):
        for n in range(3, 5):
            kv_copy(NEAR[n]).wait()
            spread(n)
    lax.fori_loop(0, 8, middle, 0)
    with jax.named_scope("spread3"):
        for n in range(5, 8):
            kv_copy(NEAR[n]).wait()
            spread(n)

    def late(i, carry):
        d = near_first(7 - i)
        best, acc = attend(d, PARTS[2], best_s[d], acc_s[d])
        osend[d, 0:HEAD_DIM, :] = acc[0:HEAD_DIM, 0:tok].astype(bf)
        osend[d, HEAD_DIM:, :] = acc[0:HEAD_DIM, tok:].astype(bf)
        mlsend[d, 0:1, :] = best
        mlsend[d, 1:2, :] = acc[HEAD_DIM:HEAD_DIM + 1, :]

        @pl.when(d > 0)
        def _():
            o_copy(d).start()
            ml_copy(d).start()

        return carry

    lax.fori_loop(0, 8, late, 0)

    def finish(d, carry):
        ml_copy(d).wait()
        o_copy(d).wait()
        return carry

    with jax.named_scope("wait_part"):
        lax.fori_loop(1, 8, finish, 0)
    with jax.named_scope("combine"):
        tops = [mlsend[0, 0:1, :]] + [mlrecv[d, 0:1, :] for d in range(1, 8)]
        top = functools.reduce(jnp.maximum, tops)
        sums = jnp.zeros_like(top)
        heads = [jnp.zeros((HEAD_DIM, tok), f32) for _ in range(2)]
        for d in range(8):
            w = jnp.exp2((tops[d] - top) * factor)
            sums = sums + w * (mlsend[0, 1:2, :] if d == 0 else mlrecv[d, 1:2, :])
            o = (osend[0] if d == 0 else orecv[d]).astype(f32)
            for h in range(2):
                heads[h] = heads[h] + o[h * HEAD_DIM:(h + 1) * HEAD_DIM, :] * w[:, h * tok:(h + 1) * tok]
        full = jnp.concatenate([heads[h] / sums[:, h * tok:(h + 1) * tok] for h in range(2)], axis=0)
        joined = full.T.astype(bf)
        for x in range(4):
            attv[x] = joined[x * rows:(x + 1) * rows, :]

    def x_copy(d):
        to = lax.rem(me_x + d, 4)
        return remote(attv.at[to], att.at[me_x], xs.at[d], xr.at[d], sp, to)

    with jax.named_scope("x_exchange"):
        for d in (2, 1, 3):
            x_copy(d).start()
        for way in range(2):
            down_copy(way).wait()
        for n in range(4):
            pass_on(n)
        att[me_x] = attv[me_x]
        weights[0].wait()
        for d in (1, 3, 2):
            x_copy(d).wait()
    with jax.named_scope("proj"):
        mixed = jnp.zeros(resid_ref.shape, f32)
        for x in range(4):
            mixed = mixed + jnp.dot(att[x], outw[x * LANES:(x + 1) * LANES, :], preferred_element_type=f32)
        residual = (resid_ref[...].astype(f32) + mixed).astype(bf)
        resid_f = residual.astype(f32)
        scale = lax.rsqrt(jnp.mean(resid_f * resid_f, axis=-1, keepdims=True) + eps)
        normed = (resid_f * scale * gain_ref[...]).astype(bf)
        resid_s[...] = residual

    with jax.named_scope("fill"):
        chosen = jnp.dot(pick[...], jnp.concatenate([normed, normed], axis=0), preferred_element_type=f32)
        sendbuf[...] = chosen.astype(bf).reshape(64, 3, 16, LANES)

    def dispatch(dz):
        def send(dj, carry):
            remote(sendbuf.at[dz * 8 + dj], recv.at[dz, dj], ss, sr.at[dz], at_offset(dz, dj), me_x).start()
            return carry

        lax.fori_loop(1 if dz == 0 else 0, 8, send, 0)

    with jax.named_scope("dispatch"):
        for dz in GROUPS[:LEAD]:
            dispatch(dz)
        recv[0, 0] = sendbuf[0]

    def a_copy(dz, way):
        return remote(
            recv.at[dz], xall.at[2 * way, dz], axs.at[way, dz], axr.at[way, dz], sp, left if way == 0 else right)

    def b_copy(dz, way):
        part = pl.ds(4 * way, 4)
        return remote(
            xall.at[2 * way, dz, part], xall.at[1, dz, part], bxs.at[way, dz], bxr.at[way, dz],
            sp, left if way == 0 else right)

    def h_copy(dz, d):
        return remote(hsend.at[d, dz], hall.at[d, dz], hs.at[d, dz], hr.at[d, dz], sp, lax.rem(me_x + d, 4))

    def stage_a(dz):
        with jax.named_scope(f"A{dz}"):
            arrived = recv.at[0, pl.ds(1, 7)] if dz == 0 else recv.at[dz]
            pltpu.make_async_copy(arrived, arrived, sr.at[dz]).wait()
            for way in range(2):
                a_copy(dz, way).start()
            after = GROUPS.index(dz) + LEAD
            if after < 8:
                dispatch(GROUPS[after])

    def stage_b(dz):
        with jax.named_scope(f"B{dz}"):
            for way in range(2):
                a_copy(dz, way).wait()
                b_copy(dz, way).start()

    def stage_c(pair):
        with jax.named_scope(f"Cw{pair[0]}"):
            for dz in pair:
                for way in range(2):
                    b_copy(dz, way).wait()
        with jax.named_scope(f"C{pair[0]}"):
            block = jnp.concatenate(
                [recv[dz].reshape(24, 16, LANES) for dz in pair]
                + [xall[d, dz].reshape(24, 16, LANES) for d in range(3) for dz in pair], axis=0)
            block = block.reshape(block.shape[0], 16 * LANES)
            gate = jnp.dot(block, gatew[...], preferred_element_type=f32)
            upper = jnp.dot(block, upw[...], preferred_element_type=f32)
            hidden = (gate / (1.0 + jnp.exp(-gate)) * upper).astype(bf)
            for n, dz in enumerate(pair):
                hall[0, dz] = hidden[24 * n:24 * (n + 1)]
                for d in range(1, 4):
                    begin = 24 * (len(pair) * d + n)
                    hsend[d, dz] = hidden[begin:begin + 24]
            for dz in pair:
                for d in range(1, 4):
                    h_copy(dz, d).start()

    def stage_d(pair):
        with jax.named_scope(f"Dw{pair[0]}"):
            for dz in pair:
                for d in range(1, 4):
                    h_copy(dz, d).wait()
        with jax.named_scope(f"D{pair[0]}"):
            full = None
            for d in range(4):
                hidden = jnp.concatenate([hall[d, dz] for dz in pair], axis=0)
                term = jnp.dot(hidden, dcat[(4 - d) % 4], preferred_element_type=f32)
                full = term if full is None else full + term
            tiles = full.astype(bf).reshape(len(pair), 8, 3, 16, LANES)
            for n, dz in enumerate(pair):
                retsend[dz] = tiles[n]
            for dz in pair:
                def give(dj, carry, dz=dz):
                    remote(
                        retsend.at[dz, dj], ret.at[pl.ds(24 * dz + 3 * dj, 3)], ts, tr,
                        at_offset(8 - dz, 8 - dj), me_x).start()
                    return carry

                if dz == 0:
                    ret[0:3] = retsend[0, 0]
                lax.fori_loop(1 if dz == 0 else 0, 8, give, 0)

    pairs = [GROUPS[n:n + 2] for n in range(0, 8, 2)]

    def wait_down():
        with jax.named_scope("wait_down"):
            weights[3].wait()
            for way in range(2):
                for n in range(4):
                    down_pass(way, n).wait()

    g = GROUPS
    stage_a(g[0])
    stage_a(g[1])
    stage_b(g[0])
    stage_a(g[2])
    stage_b(g[1])
    stage_a(g[3])
    stage_b(g[2])
    weights[1].wait()
    weights[2].wait()
    stage_c(pairs[0])
    stage_a(g[4])
    stage_b(g[3])
    stage_a(g[5])
    stage_b(g[4])
    wait_down()
    stage_d(pairs[0])
    stage_c(pairs[1])
    stage_a(g[6])
    stage_b(g[5])
    stage_a(g[7])
    stage_b(g[6])
    stage_d(pairs[1])
    stage_c(pairs[2])
    stage_c(g[6:7])
    stage_b(g[7])
    stage_d(pairs[2])
    stage_c(g[7:8])
    stage_d(g[6:7])
    stage_d(g[7:8])

    with jax.named_scope("wait_ret"):
        pltpu.make_async_copy(ret.at[pl.ds(3, 189)], ret.at[pl.ds(3, 189)], tr).wait()

    with jax.named_scope("join"):
        picked = jnp.dot(joiner[...], ret[...].reshape(192, 16 * LANES), preferred_element_type=f32)
        share = route_ref[...].T
        both = picked[0:rows] * share[:, 0:1] + picked[rows:] * share[:, 1:2]
        out_ref[...] = (resid_s[...].astype(f32) + both).astype(bf)
    pltpu.make_async_copy(sendbuf.at[pl.ds(1, 63)], sendbuf.at[pl.ds(1, 63)], ss).wait()
    pltpu.make_async_copy(sendbuf.at[pl.ds(1, 63)], sendbuf.at[pl.ds(1, 63)], ts).wait()


def body(
    resid_in,
    query_proj,
    key_proj,
    value_proj,
    query_gain,
    key_gain,
    out_weight,
    norm_gain,
    gate_weight,
    up_weight,
    down_weight,
    expert_ids,
    route_weight,
):
    tok = query_proj.shape[0]
    rows = resid_in.shape[0]
    ff = down_weight.shape[1]
    bf, f32 = jnp.bfloat16, jnp.float32
    dma = pltpu.SemaphoreType.DMA
    vmem = pl.BlockSpec(memory_space=pltpu.VMEM)
    hbm = pl.BlockSpec(memory_space=pl.ANY)
    return pl.pallas_call(
        layer_kernel,
        out_shape=jax.ShapeDtypeStruct(resid_in.shape, bf),
        in_specs=[vmem] * 9 + [hbm] * 4,
        out_specs=vmem,
        scratch_shapes=[
            pltpu.VMEM((8, tok, LANES), bf),
            pltpu.VMEM((8, tok, LANES), bf),
            pltpu.VMEM((8 * tok, LANES), bf),
            pltpu.VMEM((HEAD_DIM + 16, 8 * tok), bf),
            pltpu.VMEM((8, 1, 2 * tok), f32),
            pltpu.VMEM((8, HEAD_DIM + 16, 2 * tok), f32),
            pltpu.VMEM((8, LANES, tok), bf),
            pltpu.VMEM((8, 2, 2 * tok), f32),
            pltpu.VMEM((8, LANES, tok), bf),
            pltpu.VMEM((8, 2, 2 * tok), f32),
            pltpu.VMEM((4, rows, LANES), bf),
            pltpu.VMEM((4, rows, LANES), bf),
            pltpu.VMEM(out_weight.shape, bf),
            pltpu.VMEM(gate_weight.shape[1:], bf),
            pltpu.VMEM(up_weight.shape[1:], bf),
            pltpu.VMEM((4,) + down_weight.shape[1:], bf),
            pltpu.VMEM((192, TOPK * rows), bf),
            pltpu.VMEM((TOPK * rows, 192), bf),
            pltpu.VMEM(resid_in.shape, bf),
            pltpu.VMEM((64, 3, 16, LANES), bf),
            pltpu.VMEM((8, 8, 3, 16, LANES), bf),
            pltpu.VMEM((3, 8, 8, 3, 16, LANES), bf),
            pltpu.VMEM((4, 8, 24, ff), bf),
            pltpu.VMEM((4, 8, 24, ff), bf),
            pltpu.VMEM((8, 8, 3, 16, LANES), bf),
            pltpu.VMEM((192, 16, LANES), bf),
        ] + [dma((4,))] + [dma((8,))] * 8 + [dma((4,))] * 2 + [dma((10,))] * 2
        + [dma(()), dma((8,))] + [dma((2, 8))] * 4 + [dma((4, 8))] * 2 + [dma(())] * 2,
        compiler_params=pltpu.CompilerParams(
            collective_id=0, has_side_effects=True, vmem_limit_bytes=60 << 20),
    )(
        expert_ids.T, route_weight.T, query_proj, key_proj.T, value_proj.T, query_gain, key_gain, resid_in,
        norm_gain[None], out_weight, gate_weight[0], up_weight[0], down_weight[0],
    )


def solution(mesh):
    placed = (
        P(("sp", "tp"), None),
        P("sp", "tp"),
        P("sp", "tp"),
        P("sp", "tp"),
        P("tp", None),
        P("tp", None),
        P(),
        P(),
        P("sp", None, "tp"),
        P("sp", None, "tp"),
        P("sp", "tp", None),
        P("sp", None),
        P(("sp", "tp"), None),
    )
    return jax.shard_map(
        body, mesh=mesh, in_specs=placed, out_specs=P(("sp", "tp"), None), check_vma=False
    )
```

```python
import functools
import math

import jax
import jax.numpy as jnp
from jax import lax
from jax.experimental import pallas as pl
from jax.experimental.pallas import tpu as pltpu
from jax.sharding import PartitionSpec as P

HEAD_DIM = 64
TOPK = 2
GRID_W = 64
TOK_DEV = 256

eps = 1e-06
rope_base = 10000.0

LANES = 128
MESH = pl.DeviceIdType.MESH
NEAR = (0, 1, 7, 2, 6, 3, 5, 4)
PACE = ((0, 1, 2), (3,), (4,), (5,), (6,), (7,), (), (), ())
GROUPS = (0, 1, 5, 3, 4, 6, 2, 7)
PARTS = (((0, 512), (512, 256)), ((768, 512),), ((1280, 512), (1792, 256)))


def near_first(i):
    return lax.rem(8 + (2 * lax.rem(i, 2) - 1) * ((i + 1) // 2), 8)


def rotary_tables(sp):
    shape = (GRID_W + 8, LANES)
    freq_count = HEAD_DIM // 4
    lane = lax.broadcasted_iota(jnp.int32, shape, 1)
    item = lax.broadcasted_iota(jnp.int32, shape, 0)
    position = jnp.where(item < GRID_W, item, item - GRID_W + sp * (TOK_DEV // GRID_W)).astype(jnp.float32)
    index = lax.rem(lane, freq_count).astype(jnp.float32)
    angles = position * jnp.exp(index * (-math.log(rope_base) / freq_count))
    row_lane = lax.rem(lane[:GRID_W], 2 * freq_count) < freq_count

    def table(values):
        col = values[:GRID_W]
        return jnp.concatenate(
            [jnp.where(row_lane, values[GRID_W + r:GRID_W + r + 1], col) for r in range(TOK_DEV // GRID_W)], axis=0)

    return table(jnp.cos(angles)), table(jnp.sin(angles))


def prepare(values_f, gains, cosine, sine_table):
    lane = lax.broadcasted_iota(jnp.int32, values_f.shape, 1)
    low = lane < HEAD_DIM
    squares = values_f * values_f
    first = jnp.sum(jnp.where(low, squares, 0.0), axis=-1, keepdims=True)
    second = jnp.sum(jnp.where(low, 0.0, squares), axis=-1, keepdims=True)
    scale = jnp.where(low, lax.rsqrt(first / HEAD_DIM + eps), lax.rsqrt(second / HEAD_DIM + eps))
    normed = values_f * scale * gains
    half_dim = HEAD_DIM // 2
    turned = jnp.where(
        lax.rem(lane, HEAD_DIM) < half_dim, -pltpu.roll(normed, LANES - half_dim, 1), pltpu.roll(normed, half_dim, 1))
    return normed * cosine + turned * sine_table


def layer_kernel(
    ids_ref, route_ref, query_ref, key_ref, value_ref, qgain_ref, kgain_ref, resid_ref, gain_ref,
    outw_hbm, gate_hbm, up_hbm, down_hbm,
    out_ref,
    qall, kvall, kk, vt, best_s, acc_s, osend, mlsend, orecv, mlrecv, attv, att,
    outw, gatew, upw, dcat, pick, joiner, resid_s, sendbuf, recv, xall, hall, hsend, retsend, ret,
    wsem, qs, qr, ks, kr, ps, pr, ms, mr, xs, xr, ds, dr,
    ss, sr, axs, axr, bxs, bxr, hs, hr, ts, tr,
):
    sp = lax.axis_index("sp")
    me_x = lax.axis_index("tp")
    z, j = sp // 8, lax.rem(sp, 8)
    right, left = lax.rem(me_x + 1, 4), lax.rem(me_x + 3, 4)
    tok = query_ref.shape[0]
    rows = resid_ref.shape[0]
    bf, f32 = jnp.bfloat16, jnp.float32

    def at_offset(dz, dj):
        return lax.rem(z + dz, 8) * 8 + lax.rem(j + dj, 8)

    def remote(src, dst, send, recv_sem, sp_to, x_to):
        return pltpu.make_async_remote_copy(
            src_ref=src, dst_ref=dst, send_sem=send, recv_sem=recv_sem,
            device_id=(sp_to, x_to), device_id_type=MESH)

    barrier = pltpu.get_barrier_semaphore()

    with jax.named_scope("greet"):
        for d in range(1, 4):
            pl.semaphore_signal(barrier, inc=1, device_id=(sp, lax.rem(me_x + d, 4)), device_id_type=MESH)
        for d in range(1, 8):
            for dz, dj in ((0, d), (d, 0)):
                pl.semaphore_signal(barrier, inc=1, device_id=(at_offset(dz, dj), me_x), device_id_type=MESH)

    weights = [
        pltpu.make_async_copy(a, b, wsem.at[n])
        for n, (a, b) in enumerate(((outw_hbm, outw), (gate_hbm, gatew), (up_hbm, upw), (down_hbm, dcat.at[0])))
    ]
    for copy in weights:
        copy.start()

    with jax.named_scope("prep"):
        lane = lax.broadcasted_iota(jnp.int32, (tok, LANES), 1)
        low = lane < HEAD_DIM
        cosine, sine_table = rotary_tables(sp)
        qgain = jnp.concatenate([qgain_ref[0:1, :], qgain_ref[1:2, :]], axis=1)
        qall[0] = prepare(query_ref[...].astype(f32), qgain, cosine, sine_table).astype(bf)
        key_value = jnp.concatenate([key_ref[...].astype(f32), value_ref[...].astype(f32)], axis=0).T
        kgain = jnp.concatenate([kgain_ref[...], kgain_ref[...]], axis=1)
        kvall[0] = jnp.where(low, prepare(key_value, kgain, cosine, sine_table), key_value).astype(bf)
        vt[HEAD_DIM:, :] = jnp.ones((16, vt.shape[1]), bf)
    with jax.named_scope("barrier"):
        pl.semaphore_wait(barrier, 17)

    def q_copy(d):
        return remote(qall.at[0], qall.at[d], qs.at[d], qr.at[d], at_offset(0, d), me_x)

    def kv_copy(d):
        return remote(kvall.at[0], kvall.at[d], ks.at[d], kr.at[d], at_offset(d, 0), me_x)

    half = down_hbm.shape[0] // 2
    quarter = half // 4

    def down_copy(way):
        return remote(down_hbm, dcat.at[1 + 2 * way], ds.at[way], dr.at[way], sp, left if way == 0 else right)

    def down_pass(way, n):
        part = pl.ds(half * way + quarter * n, quarter)
        return remote(
            dcat.at[1 + 2 * way, part], dcat.at[2, part], ds.at[2 + 2 * n + way], dr.at[2 + 2 * n + way],
            sp, left if way == 0 else right)

    with jax.named_scope("issue"):
        for d in NEAR[1:3]:
            kv_copy(d).start()
        for d in NEAR[1:]:
            q_copy(d).start()
        for d in NEAR[3:5]:
            kv_copy(d).start()
        for way in range(2):
            down_copy(way).start()

    def spread(n):
        f = kvall[NEAR[n]].astype(f32)
        kk[n * tok:(n + 1) * tok, :] = jnp.where(low, f, pltpu.roll(f, HEAD_DIM, 1)).astype(bf)
        vt[0:HEAD_DIM, n * tok:(n + 1) * tok] = f.T[HEAD_DIM:, :].astype(bf)

    with jax.named_scope("routing"):
        ids = ids_ref[0:2, 0:rows]
        for x in range(1, 4):
            ids = jnp.where(me_x == x, ids_ref[0:2, x * rows:(x + 1) * rows], ids)
        ids = ids.astype(f32)
        items = TOPK * rows
        flat = jnp.broadcast_to(jnp.concatenate([ids[0:1], ids[1:2]], axis=1), (items, items))
        turned = flat.T
        same = flat == turned
        first = lax.broadcasted_iota(jnp.int32, (items, items), 0)
        second = lax.broadcasted_iota(jnp.int32, (items, items), 1)

        def slot_of(e, rank):
            e = e.astype(jnp.int32)
            place = lax.rem(lax.div(e, 8) + 8 - z, 8) * 8 + lax.rem(lax.rem(e, 8) + 8 - j, 8)
            return place * 3 + rank.astype(jnp.int32)

        across = slot_of(flat[0:1], jnp.sum(jnp.where(same & (first < second), 1.0, 0.0), axis=0, keepdims=True))
        down = slot_of(turned[:, 0:1], jnp.sum(jnp.where(same & (second < first), 1.0, 0.0), axis=1, keepdims=True))
        pick[...] = jnp.where(lax.broadcasted_iota(jnp.int32, pick.shape, 0) == across, 1.0, 0.0).astype(bf)
        joiner[...] = jnp.where(lax.broadcasted_iota(jnp.int32, joiner.shape, 1) == down, 1.0, 0.0).astype(bf)

    with jax.named_scope("spread1"):
        spread(0)
        for n in range(1, 3):
            with jax.named_scope(f"wait_kv{n}"):
                kv_copy(NEAR[n]).wait()
            if n == 1:
                for d in NEAR[5:]:
                    kv_copy(d).start()
            spread(n)

    factor = math.log2(math.e) * HEAD_DIM ** (-0.5)

    def o_copy(d):
        return remote(osend.at[d], orecv.at[d], ps.at[d], pr.at[d], at_offset(0, 8 - d), me_x)

    def ml_copy(d):
        return remote(mlsend.at[d], mlrecv.at[d], ms.at[d], mr.at[d], at_offset(0, 8 - d), me_x)

    def pass_on(n):
        for way in range(2):
            down_pass(way, n).start()

    def attend(d, spans, best, acc):
        with jax.named_scope("attend"):
            q = qall[d]
            zero = jnp.zeros_like(q)
            both = jnp.concatenate([jnp.where(low, q, zero), jnp.where(low, zero, q)], axis=0)

            def scores(span):
                return lax.dot_general(
                    kk[span[0]:span[0] + span[1], :], both, (((1,), (1,)), ((), ())), preferred_element_type=f32)

            s = scores(spans[0])
            for n, (begin, size) in enumerate(spans):
                ahead = scores(spans[n + 1]) if n + 1 < len(spans) else None
                new = jnp.max(s, axis=0, keepdims=True)
                if best is not None:
                    new = jnp.maximum(best, new)
                p = jnp.exp2((s - new) * factor).astype(bf)
                part = jnp.dot(vt[:, begin:begin + size], p, preferred_element_type=f32)
                acc = part if best is None else acc * jnp.exp2((best - new) * factor) + part
                best, s = new, ahead
            return best, acc

    def early(i, carry):
        d = near_first(i)
        with jax.named_scope("wait_q"):
            pl.when(d > 0)(lambda: q_copy(d).wait())
        best, acc = attend(d, PARTS[0], None, None)
        best_s[d] = best
        acc_s[d] = acc
        return carry

    def middle(d, carry):
        best, acc = attend(d, PARTS[1], best_s[d], acc_s[d])
        best_s[d] = best
        acc_s[d] = acc
        return carry

    lax.fori_loop(0, 8, early, 0)
    with jax.named_scope("spread2"):
        for n in range(3, 5):
            kv_copy(NEAR[n]).wait()
            spread(n)
    lax.fori_loop(0, 8, middle, 0)
    with jax.named_scope("spread3"):
        for n in range(5, 8):
            kv_copy(NEAR[n]).wait()
            spread(n)

    def late(i, carry):
        d = near_first(7 - i)
        best, acc = attend(d, PARTS[2], best_s[d], acc_s[d])
        osend[d, 0:HEAD_DIM, :] = acc[0:HEAD_DIM, 0:tok].astype(bf)
        osend[d, HEAD_DIM:, :] = acc[0:HEAD_DIM, tok:].astype(bf)
        mlsend[d, 0:1, :] = best
        mlsend[d, 1:2, :] = acc[HEAD_DIM:HEAD_DIM + 1, :]

        @pl.when(d > 0)
        def _():
            o_copy(d).start()
            ml_copy(d).start()

        return carry

    lax.fori_loop(0, 8, late, 0)
    with jax.named_scope("down_turn"):
        for way in range(2):
            down_copy(way).wait()
        pass_on(0)

    def finish(d, carry):
        ml_copy(d).wait()
        o_copy(d).wait()
        return carry

    with jax.named_scope("wait_part"):
        lax.fori_loop(1, 8, finish, 0)
    with jax.named_scope("combine"):
        tops = [mlsend[0, 0:1, :]] + [mlrecv[d, 0:1, :] for d in range(1, 8)]
        top = functools.reduce(jnp.maximum, tops)
        sums = jnp.zeros_like(top)
        heads = [jnp.zeros((HEAD_DIM, tok), f32) for _ in range(2)]
        for d in range(8):
            w = jnp.exp2((tops[d] - top) * factor)
            sums = sums + w * (mlsend[0, 1:2, :] if d == 0 else mlrecv[d, 1:2, :])
            o = (osend[0] if d == 0 else orecv[d]).astype(f32)
            for h in range(2):
                heads[h] = heads[h] + o[h * HEAD_DIM:(h + 1) * HEAD_DIM, :] * w[:, h * tok:(h + 1) * tok]
        full = jnp.concatenate([heads[h] / sums[:, h * tok:(h + 1) * tok] for h in range(2)], axis=0)
        joined = full.T.astype(bf)
        for x in range(4):
            attv[x] = joined[x * rows:(x + 1) * rows, :]

    def x_copy(d):
        to = lax.rem(me_x + d, 4)
        return remote(attv.at[to], att.at[me_x], xs.at[d], xr.at[d], sp, to)

    with jax.named_scope("x_exchange"):
        for d in (2, 1, 3):
            x_copy(d).start()
        for n in range(1, 4):
            pass_on(n)
        att[me_x] = attv[me_x]
        weights[0].wait()
        for d in (1, 3, 2):
            x_copy(d).wait()
    with jax.named_scope("proj"):
        mixed = jnp.zeros(resid_ref.shape, f32)
        for x in range(4):
            mixed = mixed + jnp.dot(att[x], outw[x * LANES:(x + 1) * LANES, :], preferred_element_type=f32)
        residual = (resid_ref[...].astype(f32) + mixed).astype(bf)
        resid_f = residual.astype(f32)
        scale = lax.rsqrt(jnp.mean(resid_f * resid_f, axis=-1, keepdims=True) + eps)
        normed = (resid_f * scale * gain_ref[...]).astype(bf)
        resid_s[...] = residual

    with jax.named_scope("fill"):
        chosen = jnp.dot(pick[...], jnp.concatenate([normed, normed], axis=0), preferred_element_type=f32)
        sendbuf[...] = chosen.astype(bf).reshape(64, 3, 16, LANES)

    def dispatch(dz):
        def send(dj, carry):
            remote(sendbuf.at[dz * 8 + dj], recv.at[dz, dj], ss, sr.at[dz], at_offset(dz, dj), me_x).start()
            return carry

        lax.fori_loop(1 if dz == 0 else 0, 8, send, 0)

    with jax.named_scope("dispatch"):
        for n in PACE[0]:
            dispatch(GROUPS[n])
        recv[0, 0] = sendbuf[0]

    def a_copy(dz, way):
        return remote(
            recv.at[dz], xall.at[2 * way, dz], axs.at[way, dz], axr.at[way, dz], sp, left if way == 0 else right)

    def b_copy(dz, way):
        part = pl.ds(4 * way, 4)
        return remote(
            xall.at[2 * way, dz, part], xall.at[1, dz, part], bxs.at[way, dz], bxr.at[way, dz],
            sp, left if way == 0 else right)

    def far_copy(dz):
        return remote(
            recv.at[dz], xall.at[1, dz], bxs.at[0, dz], bxr.at[0, dz], sp, lax.rem(me_x + 2, 4))

    def h_copy(dz, d):
        return remote(hsend.at[d, dz], hall.at[d, dz], hs.at[d, dz], hr.at[d, dz], sp, lax.rem(me_x + d, 4))

    def stage_a(dz):
        with jax.named_scope(f"A{dz}"):
            arrived = recv.at[0, pl.ds(1, 7)] if dz == 0 else recv.at[dz]
            pltpu.make_async_copy(arrived, arrived, sr.at[dz]).wait()
            for way in range(2):
                a_copy(dz, way).start()
            if dz == GROUPS[-1]:
                far_copy(dz).start()
            for n in PACE[GROUPS.index(dz) + 1]:
                dispatch(GROUPS[n])

    def stage_b(dz):
        with jax.named_scope(f"B{dz}"):
            for way in range(2):
                a_copy(dz, way).wait()
                if dz != GROUPS[-1]:
                    b_copy(dz, way).start()

    def stage_c(pair):
        with jax.named_scope(f"Cw{pair[0]}"):
            for dz in pair:
                if dz == GROUPS[-1]:
                    far_copy(dz).wait()
                else:
                    for way in range(2):
                        b_copy(dz, way).wait()
        with jax.named_scope(f"C{pair[0]}"):
            block = jnp.concatenate(
                [recv[dz].reshape(24, 16, LANES) for dz in pair]
                + [xall[d, dz].reshape(24, 16, LANES) for d in range(3) for dz in pair], axis=0)
            block = block.reshape(block.shape[0], 16 * LANES)
            gate = jnp.dot(block, gatew[...], preferred_element_type=f32)
            upper = jnp.dot(block, upw[...], preferred_element_type=f32)
            hidden = (gate / (1.0 + jnp.exp(-gate)) * upper).astype(bf)
            for n, dz in enumerate(pair):
                hall[0, dz] = hidden[24 * n:24 * (n + 1)]
                for d in range(1, 4):
                    begin = 24 * (len(pair) * d + n)
                    hsend[d, dz] = hidden[begin:begin + 24]
            for dz in pair:
                for d in range(1, 4):
                    h_copy(dz, d).start()

    def stage_d(pair):
        with jax.named_scope(f"Dw{pair[0]}"):
            for dz in pair:
                for d in range(1, 4):
                    h_copy(dz, d).wait()
        with jax.named_scope(f"D{pair[0]}"):
            full = None
            for d in range(4):
                hidden = jnp.concatenate([hall[d, dz] for dz in pair], axis=0)
                term = jnp.dot(hidden, dcat[(4 - d) % 4], preferred_element_type=f32)
                full = term if full is None else full + term
            tiles = full.astype(bf).reshape(len(pair), 8, 3, 16, LANES)
            for n, dz in enumerate(pair):
                retsend[dz] = tiles[n]
            for dz in pair:
                def give(dj, carry, dz=dz):
                    remote(
                        retsend.at[dz, dj], ret.at[pl.ds(24 * dz + 3 * dj, 3)], ts, tr,
                        at_offset(8 - dz, 8 - dj), me_x).start()
                    return carry

                if dz == 0:
                    ret[0:3] = retsend[0, 0]
                lax.fori_loop(1 if dz == 0 else 0, 8, give, 0)

    def wait_down():
        with jax.named_scope("wait_down"):
            weights[3].wait()
            for way in range(2):
                for n in range(4):
                    down_pass(way, n).wait()

    g = GROUPS
    stage_a(g[0])
    for n in range(1, 11):
        if n < 8:
            stage_a(g[n])
        if n == 2:
            weights[1].wait()
            weights[2].wait()
        if n == 3:
            wait_down()
        if n <= 8:
            stage_b(g[n - 1])
        if 2 <= n <= 9:
            stage_c(g[n - 2:n - 1])
        if 3 <= n:
            stage_d(g[n - 3:n - 2])

    with jax.named_scope("wait_ret"):
        pltpu.make_async_copy(ret.at[pl.ds(3, 189)], ret.at[pl.ds(3, 189)], tr).wait()

    with jax.named_scope("join"):
        picked = jnp.dot(joiner[...], ret[...].reshape(192, 16 * LANES), preferred_element_type=f32)
        share = route_ref[...].T
        both = picked[0:rows] * share[:, 0:1] + picked[rows:] * share[:, 1:2]
        out_ref[...] = (resid_s[...].astype(f32) + both).astype(bf)
    pltpu.make_async_copy(sendbuf.at[pl.ds(1, 63)], sendbuf.at[pl.ds(1, 63)], ss).wait()
    pltpu.make_async_copy(sendbuf.at[pl.ds(1, 63)], sendbuf.at[pl.ds(1, 63)], ts).wait()


def body(
    resid_in,
    query_proj,
    key_proj,
    value_proj,
    query_gain,
    key_gain,
    out_weight,
    norm_gain,
    gate_weight,
    up_weight,
    down_weight,
    expert_ids,
    route_weight,
):
    tok = query_proj.shape[0]
    rows = resid_in.shape[0]
    ff = down_weight.shape[1]
    bf, f32 = jnp.bfloat16, jnp.float32
    dma = pltpu.SemaphoreType.DMA
    vmem = pl.BlockSpec(memory_space=pltpu.VMEM)
    hbm = pl.BlockSpec(memory_space=pl.ANY)
    return pl.pallas_call(
        layer_kernel,
        out_shape=jax.ShapeDtypeStruct(resid_in.shape, bf),
        in_specs=[vmem] * 9 + [hbm] * 4,
        out_specs=vmem,
        scratch_shapes=[
            pltpu.VMEM((8, tok, LANES), bf),
            pltpu.VMEM((8, tok, LANES), bf),
            pltpu.VMEM((8 * tok, LANES), bf),
            pltpu.VMEM((HEAD_DIM + 16, 8 * tok), bf),
            pltpu.VMEM((8, 1, 2 * tok), f32),
            pltpu.VMEM((8, HEAD_DIM + 16, 2 * tok), f32),
            pltpu.VMEM((8, LANES, tok), bf),
            pltpu.VMEM((8, 2, 2 * tok), f32),
            pltpu.VMEM((8, LANES, tok), bf),
            pltpu.VMEM((8, 2, 2 * tok), f32),
            pltpu.VMEM((4, rows, LANES), bf),
            pltpu.VMEM((4, rows, LANES), bf),
            pltpu.VMEM(out_weight.shape, bf),
            pltpu.VMEM(gate_weight.shape[1:], bf),
            pltpu.VMEM(up_weight.shape[1:], bf),
            pltpu.VMEM((4,) + down_weight.shape[1:], bf),
            pltpu.VMEM((192, TOPK * rows), bf),
            pltpu.VMEM((TOPK * rows, 192), bf),
            pltpu.VMEM(resid_in.shape, bf),
            pltpu.VMEM((64, 3, 16, LANES), bf),
            pltpu.VMEM((8, 8, 3, 16, LANES), bf),
            pltpu.VMEM((3, 8, 8, 3, 16, LANES), bf),
            pltpu.VMEM((4, 8, 24, ff), bf),
            pltpu.VMEM((4, 8, 24, ff), bf),
            pltpu.VMEM((8, 8, 3, 16, LANES), bf),
            pltpu.VMEM((192, 16, LANES), bf),
        ] + [dma((4,))] + [dma((8,))] * 8 + [dma((4,))] * 2 + [dma((10,))] * 2
        + [dma(()), dma((8,))] + [dma((2, 8))] * 4 + [dma((4, 8))] * 2 + [dma(())] * 2,
        compiler_params=pltpu.CompilerParams(
            collective_id=0, has_side_effects=True, vmem_limit_bytes=60 << 20),
    )(
        expert_ids.T, route_weight.T, query_proj, key_proj.T, value_proj.T, query_gain, key_gain, resid_in,
        norm_gain[None], out_weight, gate_weight[0], up_weight[0], down_weight[0],
    )


def solution(mesh):
    placed = (
        P(("sp", "tp"), None),
        P("sp", "tp"),
        P("sp", "tp"),
        P("sp", "tp"),
        P("tp", None),
        P("tp", None),
        P(),
        P(),
        P("sp", None, "tp"),
        P("sp", None, "tp"),
        P("sp", "tp", None),
        P("sp", None),
        P(("sp", "tp"), None),
    )
    return jax.shard_map(
        body, mesh=mesh, in_specs=placed, out_specs=P(("sp", "tp"), None), check_vma=False
    )
```

```python
import functools
import math

import jax
import jax.numpy as jnp
from jax import lax
from jax.experimental import pallas as pl
from jax.experimental.pallas import tpu as pltpu
from jax.sharding import PartitionSpec as P

HEAD_DIM = 64
TOPK = 2
GRID_W = 64
TOK_DEV = 256

eps = 1e-06
rope_base = 10000.0

LANES = 128
MESH = pl.DeviceIdType.MESH
NEAR = (0, 1, 7, 2, 6, 3, 5, 4)
PACE = ((0, 1, 2), (3,), (4,), (5,), (6,), (7,), (), (), ())
GROUPS = (0, 1, 5, 4, 3, 6, 2, 7)
PARTS = (((0, 512), (512, 256)), ((768, 512),), ((1280, 512), (1792, 256)))


def near_first(i):
    return lax.rem(8 + (2 * lax.rem(i, 2) - 1) * ((i + 1) // 2), 8)


def rotary_tables(sp):
    shape = (GRID_W + 8, LANES)
    freq_count = HEAD_DIM // 4
    lane = lax.broadcasted_iota(jnp.int32, shape, 1)
    item = lax.broadcasted_iota(jnp.int32, shape, 0)
    position = jnp.where(item < GRID_W, item, item - GRID_W + sp * (TOK_DEV // GRID_W)).astype(jnp.float32)
    index = lax.rem(lane, freq_count).astype(jnp.float32)
    angles = position * jnp.exp(index * (-math.log(rope_base) / freq_count))
    row_lane = lax.rem(lane[:GRID_W], 2 * freq_count) < freq_count

    def table(values):
        col = values[:GRID_W]
        return jnp.concatenate(
            [jnp.where(row_lane, values[GRID_W + r:GRID_W + r + 1], col) for r in range(TOK_DEV // GRID_W)], axis=0)

    return table(jnp.cos(angles)), table(jnp.sin(angles))


def prepare(values_f, gains, cosine, sine_table):
    lane = lax.broadcasted_iota(jnp.int32, values_f.shape, 1)
    low = lane < HEAD_DIM
    squares = values_f * values_f
    first = jnp.sum(jnp.where(low, squares, 0.0), axis=-1, keepdims=True)
    second = jnp.sum(jnp.where(low, 0.0, squares), axis=-1, keepdims=True)
    scale = jnp.where(low, lax.rsqrt(first / HEAD_DIM + eps), lax.rsqrt(second / HEAD_DIM + eps))
    normed = values_f * scale * gains
    half_dim = HEAD_DIM // 2
    turned = jnp.where(
        lax.rem(lane, HEAD_DIM) < half_dim, -pltpu.roll(normed, LANES - half_dim, 1), pltpu.roll(normed, half_dim, 1))
    return normed * cosine + turned * sine_table


def layer_kernel(
    ids_in, route_in, query_in, key_in, value_in, qgain_in, kgain_in, resid_in, gain_in,
    outw_hbm, gate_hbm, up_hbm, down_hbm,
    out_ref,
    ids_ref, route_ref, query_ref, key_ref, value_ref, qgain_ref, kgain_ref, resid_ref, gain_ref, isem,
    qall, kvall, kk, vt, best_s, acc_s, osend, mlsend, orecv, mlrecv, attv, att,
    outw, gatew, upw, dcat, pick, joiner, resid_s, sendbuf, recv, xall, hall, hsend, retsend, ret,
    wsem, qs, qr, ks, kr, ps, pr, ms, mr, xs, xr, ds, dr,
    ss, sr, axs, axr, bxs, bxr, hs, hr, ts, tr,
):
    sp = lax.axis_index("sp")
    me_x = lax.axis_index("tp")
    z, j = sp // 8, lax.rem(sp, 8)
    right, left = lax.rem(me_x + 1, 4), lax.rem(me_x + 3, 4)
    tok = query_ref.shape[0]
    rows = resid_ref.shape[0]
    bf, f32 = jnp.bfloat16, jnp.float32

    def at_offset(dz, dj):
        return lax.rem(z + dz, 8) * 8 + lax.rem(j + dj, 8)

    def remote(src, dst, send, recv_sem, sp_to, x_to):
        return pltpu.make_async_remote_copy(
            src_ref=src, dst_ref=dst, send_sem=send, recv_sem=recv_sem,
            device_id=(sp_to, x_to), device_id_type=MESH)

    barrier = pltpu.get_barrier_semaphore()

    with jax.named_scope("greet"):
        for d in range(1, 4):
            pl.semaphore_signal(barrier, inc=1, device_id=(sp, lax.rem(me_x + d, 4)), device_id_type=MESH)
        for d in range(1, 8):
            for dz, dj in ((0, d), (d, 0)):
                pl.semaphore_signal(barrier, inc=1, device_id=(at_offset(dz, dj), me_x), device_id_type=MESH)

    small = [
        pltpu.make_async_copy(a, b, isem.at[n])
        for n, (a, b) in enumerate((
            (query_in, query_ref), (key_in, key_ref), (value_in, value_ref), (qgain_in, qgain_ref),
            (kgain_in, kgain_ref), (ids_in, ids_ref), (route_in, route_ref), (resid_in, resid_ref), (gain_in, gain_ref)))
    ]
    for copy in small:
        copy.start()
    weights = [
        pltpu.make_async_copy(a, b, wsem.at[n])
        for n, (a, b) in enumerate(((outw_hbm, outw), (gate_hbm, gatew), (up_hbm, upw), (down_hbm, dcat.at[0])))
    ]
    for copy in weights:
        copy.start()

    with jax.named_scope("prep"):
        lane = lax.broadcasted_iota(jnp.int32, (tok, LANES), 1)
        low = lane < HEAD_DIM
        cosine, sine_table = rotary_tables(sp)
        for copy in small:
            copy.wait()
        qgain = jnp.concatenate([qgain_ref[0:1, :], qgain_ref[1:2, :]], axis=1)
        qall[0] = prepare(query_ref[...].astype(f32), qgain, cosine, sine_table).astype(bf)
        key_value = jnp.concatenate([key_ref[...].astype(f32), value_ref[...].astype(f32)], axis=0).T
        kgain = jnp.concatenate([kgain_ref[...], kgain_ref[...]], axis=1)
        kvall[0] = jnp.where(low, prepare(key_value, kgain, cosine, sine_table), key_value).astype(bf)
        vt[HEAD_DIM:, :] = jnp.ones((16, vt.shape[1]), bf)
    with jax.named_scope("barrier"):
        pl.semaphore_wait(barrier, 17)

    def q_copy(d):
        return remote(qall.at[0], qall.at[d], qs.at[d], qr.at[d], at_offset(0, d), me_x)

    def kv_copy(d):
        return remote(kvall.at[0], kvall.at[d], ks.at[d], kr.at[d], at_offset(d, 0), me_x)

    half = down_hbm.shape[0] // 2
    quarter = half // 4

    def down_copy(way):
        return remote(down_hbm, dcat.at[1 + 2 * way], ds.at[way], dr.at[way], sp, left if way == 0 else right)

    def down_pass(way, n):
        part = pl.ds(half * way + quarter * n, quarter)
        return remote(
            dcat.at[1 + 2 * way, part], dcat.at[2, part], ds.at[2 + 2 * n + way], dr.at[2 + 2 * n + way],
            sp, left if way == 0 else right)

    with jax.named_scope("issue"):
        for d in NEAR[1:3]:
            kv_copy(d).start()
        for d in NEAR[1:]:
            q_copy(d).start()
        for d in NEAR[3:5]:
            kv_copy(d).start()
        for way in range(2):
            down_copy(way).start()

    def spread(n):
        f = kvall[NEAR[n]].astype(f32)
        kk[n * tok:(n + 1) * tok, :] = jnp.where(low, f, pltpu.roll(f, HEAD_DIM, 1)).astype(bf)
        vt[0:HEAD_DIM, n * tok:(n + 1) * tok] = f.T[HEAD_DIM:, :].astype(bf)

    with jax.named_scope("routing"):
        ids = ids_ref[0:2, 0:rows]
        for x in range(1, 4):
            ids = jnp.where(me_x == x, ids_ref[0:2, x * rows:(x + 1) * rows], ids)
        ids = ids.astype(f32)
        items = TOPK * rows
        flat = jnp.broadcast_to(jnp.concatenate([ids[0:1], ids[1:2]], axis=1), (items, items))
        turned = flat.T
        same = flat == turned
        first = lax.broadcasted_iota(jnp.int32, (items, items), 0)
        second = lax.broadcasted_iota(jnp.int32, (items, items), 1)

        def slot_of(e, rank):
            e = e.astype(jnp.int32)
            place = lax.rem(lax.div(e, 8) + 8 - z, 8) * 8 + lax.rem(lax.rem(e, 8) + 8 - j, 8)
            return place * 3 + rank.astype(jnp.int32)

        across = slot_of(flat[0:1], jnp.sum(jnp.where(same & (first < second), 1.0, 0.0), axis=0, keepdims=True))
        down = slot_of(turned[:, 0:1], jnp.sum(jnp.where(same & (second < first), 1.0, 0.0), axis=1, keepdims=True))
        pick[...] = jnp.where(lax.broadcasted_iota(jnp.int32, pick.shape, 0) == across, 1.0, 0.0).astype(bf)
        joiner[...] = jnp.where(lax.broadcasted_iota(jnp.int32, joiner.shape, 1) == down, 1.0, 0.0).astype(bf)

    with jax.named_scope("spread1"):
        spread(0)
        for n in range(1, 3):
            with jax.named_scope(f"wait_kv{n}"):
                kv_copy(NEAR[n]).wait()
            if n == 1:
                for d in NEAR[5:]:
                    kv_copy(d).start()
            spread(n)

    factor = math.log2(math.e) * HEAD_DIM ** (-0.5)

    def o_copy(d):
        return remote(osend.at[d], orecv.at[d], ps.at[d], pr.at[d], at_offset(0, 8 - d), me_x)

    def ml_copy(d):
        return remote(mlsend.at[d], mlrecv.at[d], ms.at[d], mr.at[d], at_offset(0, 8 - d), me_x)

    def pass_on(n):
        for way in range(2):
            down_pass(way, n).start()

    def attend(d, spans, best, acc):
        with jax.named_scope("attend"):
            q = qall[d]
            zero = jnp.zeros_like(q)
            both = jnp.concatenate([jnp.where(low, q, zero), jnp.where(low, zero, q)], axis=0)

            def scores(span):
                return lax.dot_general(
                    kk[span[0]:span[0] + span[1], :], both, (((1,), (1,)), ((), ())), preferred_element_type=f32)

            s = scores(spans[0])
            for n, (begin, size) in enumerate(spans):
                ahead = scores(spans[n + 1]) if n + 1 < len(spans) else None
                new = jnp.max(s, axis=0, keepdims=True)
                if best is not None:
                    new = jnp.maximum(best, new)
                p = jnp.exp2((s - new) * factor).astype(bf)
                part = jnp.dot(vt[:, begin:begin + size], p, preferred_element_type=f32)
                acc = part if best is None else acc * jnp.exp2((best - new) * factor) + part
                best, s = new, ahead
            return best, acc

    def early(i, carry):
        d = near_first(i)
        with jax.named_scope("wait_q"):
            pl.when(d > 0)(lambda: q_copy(d).wait())
        best, acc = attend(d, PARTS[0], None, None)
        best_s[d] = best
        acc_s[d] = acc
        return carry

    def middle(d, carry):
        best, acc = attend(d, PARTS[1], best_s[d], acc_s[d])
        best_s[d] = best
        acc_s[d] = acc
        return carry

    lax.fori_loop(0, 8, early, 0)
    with jax.named_scope("spread2"):
        for n in range(3, 5):
            kv_copy(NEAR[n]).wait()
            spread(n)
    lax.fori_loop(0, 8, middle, 0)
    with jax.named_scope("spread3"):
        for n in range(5, 8):
            kv_copy(NEAR[n]).wait()
            spread(n)

    def late(i, carry):
        d = near_first(7 - i)
        best, acc = attend(d, PARTS[2], best_s[d], acc_s[d])
        osend[d, 0:HEAD_DIM, :] = acc[0:HEAD_DIM, 0:tok].astype(bf)
        osend[d, HEAD_DIM:, :] = acc[0:HEAD_DIM, tok:].astype(bf)
        mlsend[d, 0:1, :] = best
        mlsend[d, 1:2, :] = acc[HEAD_DIM:HEAD_DIM + 1, :]

        @pl.when(d > 0)
        def _():
            o_copy(d).start()
            ml_copy(d).start()

        return carry

    lax.fori_loop(0, 8, late, 0)

    def finish(d, carry):
        ml_copy(d).wait()
        o_copy(d).wait()
        return carry

    with jax.named_scope("wait_part"):
        lax.fori_loop(1, 8, finish, 0)
    with jax.named_scope("combine"):
        tops = [mlsend[0, 0:1, :]] + [mlrecv[d, 0:1, :] for d in range(1, 8)]
        top = functools.reduce(jnp.maximum, tops)
        sums = jnp.zeros_like(top)
        heads = [jnp.zeros((HEAD_DIM, tok), f32) for _ in range(2)]
        for d in range(8):
            w = jnp.exp2((tops[d] - top) * factor)
            sums = sums + w * (mlsend[0, 1:2, :] if d == 0 else mlrecv[d, 1:2, :])
            o = (osend[0] if d == 0 else orecv[d]).astype(f32)
            for h in range(2):
                heads[h] = heads[h] + o[h * HEAD_DIM:(h + 1) * HEAD_DIM, :] * w[:, h * tok:(h + 1) * tok]
        full = jnp.concatenate([heads[h] / sums[:, h * tok:(h + 1) * tok] for h in range(2)], axis=0)
        joined = full.T.astype(bf)
        for x in range(4):
            attv[x] = joined[x * rows:(x + 1) * rows, :]

    def x_copy(d):
        to = lax.rem(me_x + d, 4)
        return remote(attv.at[to], att.at[me_x], xs.at[d], xr.at[d], sp, to)

    with jax.named_scope("x_exchange"):
        for d in (2, 1, 3):
            x_copy(d).start()
        for way in range(2):
            down_copy(way).wait()
        for n in range(4):
            pass_on(n)
        att[me_x] = attv[me_x]
        weights[0].wait()
        for d in (1, 3, 2):
            x_copy(d).wait()
    with jax.named_scope("proj"):
        mixed = jnp.zeros(resid_ref.shape, f32)
        for x in range(4):
            mixed = mixed + jnp.dot(att[x], outw[x * LANES:(x + 1) * LANES, :], preferred_element_type=f32)
        residual = (resid_ref[...].astype(f32) + mixed).astype(bf)
        resid_f = residual.astype(f32)
        scale = lax.rsqrt(jnp.mean(resid_f * resid_f, axis=-1, keepdims=True) + eps)
        normed = (resid_f * scale * gain_ref[...]).astype(bf)
        resid_s[...] = residual

    with jax.named_scope("fill"):
        chosen = jnp.dot(pick[...], jnp.concatenate([normed, normed], axis=0), preferred_element_type=f32)
        sendbuf[...] = chosen.astype(bf).reshape(64, 3, 16, LANES)

    def dispatch(dz):
        def send(dj, carry):
            remote(sendbuf.at[dz * 8 + dj], recv.at[dz, dj], ss, sr.at[dz], at_offset(dz, dj), me_x).start()
            return carry

        lax.fori_loop(1 if dz == 0 else 0, 8, send, 0)

    with jax.named_scope("dispatch"):
        for n in PACE[0]:
            dispatch(GROUPS[n])
        recv[0, 0] = sendbuf[0]

    def a_copy(dz, way):
        return remote(
            recv.at[dz], xall.at[2 * way, dz], axs.at[way, dz], axr.at[way, dz], sp, left if way == 0 else right)

    def b_copy(dz, way):
        part = pl.ds(4 * way, 4)
        return remote(
            xall.at[2 * way, dz, part], xall.at[1, dz, part], bxs.at[way, dz], bxr.at[way, dz],
            sp, left if way == 0 else right)

    def h_copy(dz, d):
        return remote(hsend.at[d, dz], hall.at[d, dz], hs.at[d, dz], hr.at[d, dz], sp, lax.rem(me_x + d, 4))

    def stage_a(dz):
        with jax.named_scope(f"A{dz}"):
            arrived = recv.at[0, pl.ds(1, 7)] if dz == 0 else recv.at[dz]
            pltpu.make_async_copy(arrived, arrived, sr.at[dz]).wait()
            for way in range(2):
                a_copy(dz, way).start()
            for n in PACE[GROUPS.index(dz) + 1]:
                dispatch(GROUPS[n])

    def stage_b(dz):
        with jax.named_scope(f"B{dz}"):
            for way in range(2):
                a_copy(dz, way).wait()
                b_copy(dz, way).start()

    def stage_c(pair):
        with jax.named_scope(f"Cw{pair[0]}"):
            for dz in pair:
                for way in range(2):
                    b_copy(dz, way).wait()
        with jax.named_scope(f"C{pair[0]}"):
            block = jnp.concatenate(
                [recv[dz].reshape(24, 16, LANES) for dz in pair]
                + [xall[d, dz].reshape(24, 16, LANES) for d in range(3) for dz in pair], axis=0)
            block = block.reshape(block.shape[0], 16 * LANES)
            gate = jnp.dot(block, gatew[...], preferred_element_type=f32)
            upper = jnp.dot(block, upw[...], preferred_element_type=f32)
            hidden = (gate / (1.0 + jnp.exp(-gate)) * upper).astype(bf)
            for n, dz in enumerate(pair):
                hall[0, dz] = hidden[24 * n:24 * (n + 1)]
                for d in range(1, 4):
                    begin = 24 * (len(pair) * d + n)
                    hsend[d, dz] = hidden[begin:begin + 24]
            for dz in pair:
                for d in range(1, 4):
                    h_copy(dz, d).start()

    def stage_d(pair):
        with jax.named_scope(f"Dw{pair[0]}"):
            for dz in pair:
                for d in range(1, 4):
                    h_copy(dz, d).wait()
        with jax.named_scope(f"D{pair[0]}"):
            full = None
            for d in range(4):
                hidden = jnp.concatenate([hall[d, dz] for dz in pair], axis=0)
                term = jnp.dot(hidden, dcat[(4 - d) % 4], preferred_element_type=f32)
                full = term if full is None else full + term
            tiles = full.astype(bf).reshape(len(pair), 8, 3, 16, LANES)
            for n, dz in enumerate(pair):
                retsend[dz] = tiles[n]
            for dz in pair:
                def give(dj, carry, dz=dz):
                    remote(
                        retsend.at[dz, dj], ret.at[pl.ds(24 * dz + 3 * dj, 3)], ts, tr,
                        at_offset(8 - dz, 8 - dj), me_x).start()
                    return carry

                if dz == 0:
                    ret[0:3] = retsend[0, 0]
                lax.fori_loop(1 if dz == 0 else 0, 8, give, 0)

    def wait_down():
        with jax.named_scope("wait_down"):
            weights[3].wait()
            for way in range(2):
                for n in range(4):
                    down_pass(way, n).wait()

    g = GROUPS
    stage_a(g[0])
    for n in range(1, 11):
        if n < 8:
            stage_a(g[n])
        if n == 2:
            weights[1].wait()
            weights[2].wait()
        if n == 3:
            wait_down()
        if n <= 8:
            stage_b(g[n - 1])
        if 2 <= n <= 9:
            stage_c(g[n - 2:n - 1])
        if 3 <= n:
            stage_d(g[n - 3:n - 2])

    with jax.named_scope("wait_ret"):
        pltpu.make_async_copy(ret.at[pl.ds(3, 189)], ret.at[pl.ds(3, 189)], tr).wait()

    with jax.named_scope("join"):
        picked = jnp.dot(joiner[...], ret[...].reshape(192, 16 * LANES), preferred_element_type=f32)
        share = route_ref[...].T
        both = picked[0:rows] * share[:, 0:1] + picked[rows:] * share[:, 1:2]
        out_ref[...] = (resid_s[...].astype(f32) + both).astype(bf)
    pltpu.make_async_copy(sendbuf.at[pl.ds(1, 63)], sendbuf.at[pl.ds(1, 63)], ss).wait()
    pltpu.make_async_copy(sendbuf.at[pl.ds(1, 63)], sendbuf.at[pl.ds(1, 63)], ts).wait()


def body(
    resid_in,
    query_proj,
    key_proj,
    value_proj,
    query_gain,
    key_gain,
    out_weight,
    norm_gain,
    gate_weight,
    up_weight,
    down_weight,
    expert_ids,
    route_weight,
):
    tok = query_proj.shape[0]
    rows = resid_in.shape[0]
    ff = down_weight.shape[1]
    bf, f32 = jnp.bfloat16, jnp.float32
    dma = pltpu.SemaphoreType.DMA
    vmem = pl.BlockSpec(memory_space=pltpu.VMEM)
    hbm = pl.BlockSpec(memory_space=pl.ANY)
    return pl.pallas_call(
        layer_kernel,
        out_shape=jax.ShapeDtypeStruct(resid_in.shape, bf),
        in_specs=[hbm] * 13,
        out_specs=vmem,
        scratch_shapes=[
            pltpu.VMEM((TOPK, tok), jnp.int32),
            pltpu.VMEM((TOPK, rows), f32),
            pltpu.VMEM(query_proj.shape, bf),
            pltpu.VMEM(key_proj.shape[::-1], bf),
            pltpu.VMEM(value_proj.shape[::-1], bf),
            pltpu.VMEM(query_gain.shape, f32),
            pltpu.VMEM(key_gain.shape, f32),
            pltpu.VMEM(resid_in.shape, bf),
            pltpu.VMEM((1,) + norm_gain.shape, f32),
            dma((9,)),
            pltpu.VMEM((8, tok, LANES), bf),
            pltpu.VMEM((8, tok, LANES), bf),
            pltpu.VMEM((8 * tok, LANES), bf),
            pltpu.VMEM((HEAD_DIM + 16, 8 * tok), bf),
            pltpu.VMEM((8, 1, 2 * tok), f32),
            pltpu.VMEM((8, HEAD_DIM + 16, 2 * tok), f32),
            pltpu.VMEM((8, LANES, tok), bf),
            pltpu.VMEM((8, 2, 2 * tok), f32),
            pltpu.VMEM((8, LANES, tok), bf),
            pltpu.VMEM((8, 2, 2 * tok), f32),
            pltpu.VMEM((4, rows, LANES), bf),
            pltpu.VMEM((4, rows, LANES), bf),
            pltpu.VMEM(out_weight.shape, bf),
            pltpu.VMEM(gate_weight.shape[1:], bf),
            pltpu.VMEM(up_weight.shape[1:], bf),
            pltpu.VMEM((4,) + down_weight.shape[1:], bf),
            pltpu.VMEM((192, TOPK * rows), bf),
            pltpu.VMEM((TOPK * rows, 192), bf),
            pltpu.VMEM(resid_in.shape, bf),
            pltpu.VMEM((64, 3, 16, LANES), bf),
            pltpu.VMEM((8, 8, 3, 16, LANES), bf),
            pltpu.VMEM((3, 8, 8, 3, 16, LANES), bf),
            pltpu.VMEM((4, 8, 24, ff), bf),
            pltpu.VMEM((4, 8, 24, ff), bf),
            pltpu.VMEM((8, 8, 3, 16, LANES), bf),
            pltpu.VMEM((192, 16, LANES), bf),
        ] + [dma((4,))] + [dma((8,))] * 8 + [dma((4,))] * 2 + [dma((10,))] * 2
        + [dma(()), dma((8,))] + [dma((2, 8))] * 4 + [dma((4, 8))] * 2 + [dma(())] * 2,
        compiler_params=pltpu.CompilerParams(
            collective_id=0, has_side_effects=True, vmem_limit_bytes=67_000_000),
    )(
        expert_ids.T, route_weight.T, query_proj, key_proj.T, value_proj.T, query_gain, key_gain, resid_in,
        norm_gain[None], out_weight, gate_weight[0], up_weight[0], down_weight[0],
    )


def solution(mesh):
    placed = (
        P(("sp", "tp"), None),
        P("sp", "tp"),
        P("sp", "tp"),
        P("sp", "tp"),
        P("tp", None),
        P("tp", None),
        P(),
        P(),
        P("sp", None, "tp"),
        P("sp", None, "tp"),
        P("sp", "tp", None),
        P("sp", None),
        P(("sp", "tp"), None),
    )
    return jax.shard_map(
        body, mesh=mesh, in_specs=placed, out_specs=P(("sp", "tp"), None), check_vma=False
    )
```

```python
import functools
import math

import jax
import jax.numpy as jnp
from jax import lax
from jax.experimental import pallas as pl
from jax.experimental.pallas import tpu as pltpu
from jax.sharding import PartitionSpec as P

HEAD_DIM = 64
TOPK = 2
GRID_W = 64
TOK_DEV = 256

eps = 1e-06
rope_base = 10000.0

LANES = 128
MESH = pl.DeviceIdType.MESH
NEAR = (0, 1, 7, 2, 6, 3, 5, 4)
PACE = ((0, 1, 2), (3, 4), (5,), (6,), (7,), (), (), (), ())
GROUPS = (0, 1, 5, 4, 3, 6, 2, 7)
PARTS = (((0, 512), (512, 256)), ((768, 512),), ((1280, 512), (1792, 256)))


def near_first(i):
    return lax.rem(8 + (2 * lax.rem(i, 2) - 1) * ((i + 1) // 2), 8)


def rotary_tables(sp):
    shape = (GRID_W + 8, LANES)
    freq_count = HEAD_DIM // 4
    lane = lax.broadcasted_iota(jnp.int32, shape, 1)
    item = lax.broadcasted_iota(jnp.int32, shape, 0)
    position = jnp.where(item < GRID_W, item, item - GRID_W + sp * (TOK_DEV // GRID_W)).astype(jnp.float32)
    index = lax.rem(lane, freq_count).astype(jnp.float32)
    angles = position * jnp.exp(index * (-math.log(rope_base) / freq_count))
    row_lane = lax.rem(lane[:GRID_W], 2 * freq_count) < freq_count

    def table(values):
        col = values[:GRID_W]
        return jnp.concatenate(
            [jnp.where(row_lane, values[GRID_W + r:GRID_W + r + 1], col) for r in range(TOK_DEV // GRID_W)], axis=0)

    return table(jnp.cos(angles)), table(jnp.sin(angles))


def prepare(values_f, gains, cosine, sine_table):
    lane = lax.broadcasted_iota(jnp.int32, values_f.shape, 1)
    low = lane < HEAD_DIM
    squares = values_f * values_f
    first = jnp.sum(jnp.where(low, squares, 0.0), axis=-1, keepdims=True)
    second = jnp.sum(jnp.where(low, 0.0, squares), axis=-1, keepdims=True)
    scale = jnp.where(low, lax.rsqrt(first / HEAD_DIM + eps), lax.rsqrt(second / HEAD_DIM + eps))
    normed = values_f * scale * gains
    half_dim = HEAD_DIM // 2
    turned = jnp.where(
        lax.rem(lane, HEAD_DIM) < half_dim, -pltpu.roll(normed, LANES - half_dim, 1), pltpu.roll(normed, half_dim, 1))
    return normed * cosine + turned * sine_table


def layer_kernel(
    ids_in, route_in, query_in, key_in, value_in, qgain_in, kgain_in, resid_in, gain_in,
    outw_hbm, gate_hbm, up_hbm, down_hbm,
    out_ref,
    ids_ref, route_ref, query_ref, key_ref, value_ref, qgain_ref, kgain_ref, resid_ref, gain_ref, isem,
    qall, kvall, kk, vt, best_s, acc_s, osend, mlsend, orecv, mlrecv, attv, att,
    outw, gatew, upw, dcat, pick, joiner, resid_s, sendbuf, recv, xall, hall, hsend, retsend, ret,
    wsem, qs, qr, ks, kr, ps, pr, ms, mr, xs, xr, ds, dr,
    ss, sr, axs, axr, bxs, bxr, hs, hr, ts, tr,
):
    sp = lax.axis_index("sp")
    me_x = lax.axis_index("tp")
    z, j = sp // 8, lax.rem(sp, 8)
    right, left = lax.rem(me_x + 1, 4), lax.rem(me_x + 3, 4)
    tok = query_ref.shape[0]
    rows = resid_ref.shape[0]
    bf, f32 = jnp.bfloat16, jnp.float32

    def at_offset(dz, dj):
        return lax.rem(z + dz, 8) * 8 + lax.rem(j + dj, 8)

    def remote(src, dst, send, recv_sem, sp_to, x_to):
        return pltpu.make_async_remote_copy(
            src_ref=src, dst_ref=dst, send_sem=send, recv_sem=recv_sem,
            device_id=(sp_to, x_to), device_id_type=MESH)

    barrier = pltpu.get_barrier_semaphore()

    with jax.named_scope("greet"):
        for d in range(1, 4):
            pl.semaphore_signal(barrier, inc=1, device_id=(sp, lax.rem(me_x + d, 4)), device_id_type=MESH)
        for d in range(1, 8):
            for dz, dj in ((0, d), (d, 0)):
                pl.semaphore_signal(barrier, inc=1, device_id=(at_offset(dz, dj), me_x), device_id_type=MESH)

    small = [
        pltpu.make_async_copy(a, b, isem.at[n])
        for n, (a, b) in enumerate((
            (query_in, query_ref), (key_in, key_ref), (value_in, value_ref), (qgain_in, qgain_ref),
            (kgain_in, kgain_ref), (ids_in, ids_ref), (route_in, route_ref), (resid_in, resid_ref), (gain_in, gain_ref)))
    ]
    for copy in small:
        copy.start()
    weights = [
        pltpu.make_async_copy(a, b, wsem.at[n])
        for n, (a, b) in enumerate(((outw_hbm, outw), (gate_hbm, gatew), (up_hbm, upw), (down_hbm, dcat.at[0])))
    ]
    for copy in weights:
        copy.start()

    with jax.named_scope("prep"):
        lane = lax.broadcasted_iota(jnp.int32, (tok, LANES), 1)
        low = lane < HEAD_DIM
        cosine, sine_table = rotary_tables(sp)
        for copy in small:
            copy.wait()
        qgain = jnp.concatenate([qgain_ref[0:1, :], qgain_ref[1:2, :]], axis=1)
        qall[0] = prepare(query_ref[...].astype(f32), qgain, cosine, sine_table).astype(bf)
        key_value = jnp.concatenate([key_ref[...].astype(f32), value_ref[...].astype(f32)], axis=0).T
        kgain = jnp.concatenate([kgain_ref[...], kgain_ref[...]], axis=1)
        kvall[0] = jnp.where(low, prepare(key_value, kgain, cosine, sine_table), key_value).astype(bf)
        vt[HEAD_DIM:, :] = jnp.ones((16, vt.shape[1]), bf)
    with jax.named_scope("barrier"):
        pl.semaphore_wait(barrier, 17)

    def q_copy(d):
        return remote(qall.at[0], qall.at[d], qs.at[d], qr.at[d], at_offset(0, d), me_x)

    def kv_copy(d):
        return remote(kvall.at[0], kvall.at[d], ks.at[d], kr.at[d], at_offset(d, 0), me_x)

    half = down_hbm.shape[0] // 2
    quarter = half // 4

    def down_copy(way):
        return remote(down_hbm, dcat.at[1 + 2 * way], ds.at[way], dr.at[way], sp, left if way == 0 else right)

    def down_pass(way, n):
        part = pl.ds(half * way + quarter * n, quarter)
        return remote(
            dcat.at[1 + 2 * way, part], dcat.at[2, part], ds.at[2 + 2 * n + way], dr.at[2 + 2 * n + way],
            sp, left if way == 0 else right)

    with jax.named_scope("issue"):
        for d in NEAR[1:3]:
            kv_copy(d).start()
        for d in NEAR[1:]:
            q_copy(d).start()
        for d in NEAR[3:5]:
            kv_copy(d).start()
        for way in range(2):
            down_copy(way).start()

    def spread(n):
        f = kvall[NEAR[n]].astype(f32)
        kk[n * tok:(n + 1) * tok, :] = jnp.where(low, f, pltpu.roll(f, HEAD_DIM, 1)).astype(bf)
        vt[0:HEAD_DIM, n * tok:(n + 1) * tok] = f.T[HEAD_DIM:, :].astype(bf)

    with jax.named_scope("routing"):
        ids = ids_ref[0:2, 0:rows]
        for x in range(1, 4):
            ids = jnp.where(me_x == x, ids_ref[0:2, x * rows:(x + 1) * rows], ids)
        ids = ids.astype(f32)
        items = TOPK * rows
        flat = jnp.broadcast_to(jnp.concatenate([ids[0:1], ids[1:2]], axis=1), (items, items))
        turned = flat.T
        same = flat == turned
        first = lax.broadcasted_iota(jnp.int32, (items, items), 0)
        second = lax.broadcasted_iota(jnp.int32, (items, items), 1)

        def slot_of(e, rank):
            e = e.astype(jnp.int32)
            place = lax.rem(lax.div(e, 8) + 8 - z, 8) * 8 + lax.rem(lax.rem(e, 8) + 8 - j, 8)
            return place * 3 + rank.astype(jnp.int32)

        across = slot_of(flat[0:1], jnp.sum(jnp.where(same & (first < second), 1.0, 0.0), axis=0, keepdims=True))
        down = slot_of(turned[:, 0:1], jnp.sum(jnp.where(same & (second < first), 1.0, 0.0), axis=1, keepdims=True))
        pick[...] = jnp.where(lax.broadcasted_iota(jnp.int32, pick.shape, 0) == across, 1.0, 0.0).astype(bf)
        joiner[...] = jnp.where(lax.broadcasted_iota(jnp.int32, joiner.shape, 1) == down, 1.0, 0.0).astype(bf)

    with jax.named_scope("spread1"):
        spread(0)
        for n in range(1, 3):
            with jax.named_scope(f"wait_kv{n}"):
                kv_copy(NEAR[n]).wait()
            if n == 1:
                for d in NEAR[5:]:
                    kv_copy(d).start()
            spread(n)

    factor = math.log2(math.e) * HEAD_DIM ** (-0.5)

    def o_copy(d):
        return remote(osend.at[d], orecv.at[d], ps.at[d], pr.at[d], at_offset(0, 8 - d), me_x)

    def ml_copy(d):
        return remote(mlsend.at[d], mlrecv.at[d], ms.at[d], mr.at[d], at_offset(0, 8 - d), me_x)

    def pass_on(n):
        for way in range(2):
            down_pass(way, n).start()

    def attend(d, spans, best, acc):
        with jax.named_scope("attend"):
            q = qall[d]
            zero = jnp.zeros_like(q)
            both = jnp.concatenate([jnp.where(low, q, zero), jnp.where(low, zero, q)], axis=0)

            def scores(span):
                return lax.dot_general(
                    kk[span[0]:span[0] + span[1], :], both, (((1,), (1,)), ((), ())), preferred_element_type=f32)

            s = scores(spans[0])
            for n, (begin, size) in enumerate(spans):
                ahead = scores(spans[n + 1]) if n + 1 < len(spans) else None
                new = jnp.max(s, axis=0, keepdims=True)
                if best is not None:
                    new = jnp.maximum(best, new)
                p = jnp.exp2((s - new) * factor).astype(bf)
                part = jnp.dot(vt[:, begin:begin + size], p, preferred_element_type=f32)
                acc = part if best is None else acc * jnp.exp2((best - new) * factor) + part
                best, s = new, ahead
            return best, acc

    def early(i, carry):
        d = near_first(i)
        with jax.named_scope("wait_q"):
            pl.when(d > 0)(lambda: q_copy(d).wait())
        best, acc = attend(d, PARTS[0], None, None)
        best_s[d] = best
        acc_s[d] = acc
        return carry

    def middle(d, carry):
        best, acc = attend(d, PARTS[1], best_s[d], acc_s[d])
        best_s[d] = best
        acc_s[d] = acc
        return carry

    lax.fori_loop(0, 8, early, 0)
    with jax.named_scope("spread2"):
        for n in range(3, 5):
            kv_copy(NEAR[n]).wait()
            spread(n)
    lax.fori_loop(0, 8, middle, 0)
    with jax.named_scope("spread3"):
        for n in range(5, 8):
            kv_copy(NEAR[n]).wait()
            spread(n)

    def late(i, carry):
        d = near_first(7 - i)
        best, acc = attend(d, PARTS[2], best_s[d], acc_s[d])
        osend[d, 0:HEAD_DIM, :] = acc[0:HEAD_DIM, 0:tok].astype(bf)
        osend[d, HEAD_DIM:, :] = acc[0:HEAD_DIM, tok:].astype(bf)
        mlsend[d, 0:1, :] = best
        mlsend[d, 1:2, :] = acc[HEAD_DIM:HEAD_DIM + 1, :]

        @pl.when(d > 0)
        def _():
            o_copy(d).start()
            ml_copy(d).start()

        return carry

    lax.fori_loop(0, 8, late, 0)

    def finish(d, carry):
        ml_copy(d).wait()
        o_copy(d).wait()
        return carry

    with jax.named_scope("wait_part"):
        lax.fori_loop(1, 8, finish, 0)
    with jax.named_scope("combine"):
        tops = [mlsend[0, 0:1, :]] + [mlrecv[d, 0:1, :] for d in range(1, 8)]
        top = functools.reduce(jnp.maximum, tops)
        sums = jnp.zeros_like(top)
        heads = [jnp.zeros((HEAD_DIM, tok), f32) for _ in range(2)]
        for d in range(8):
            w = jnp.exp2((tops[d] - top) * factor)
            sums = sums + w * (mlsend[0, 1:2, :] if d == 0 else mlrecv[d, 1:2, :])
            o = (osend[0] if d == 0 else orecv[d]).astype(f32)
            for h in range(2):
                heads[h] = heads[h] + o[h * HEAD_DIM:(h + 1) * HEAD_DIM, :] * w[:, h * tok:(h + 1) * tok]
        full = jnp.concatenate([heads[h] / sums[:, h * tok:(h + 1) * tok] for h in range(2)], axis=0)
        joined = full.T.astype(bf)
        for x in range(4):
            attv[x] = joined[x * rows:(x + 1) * rows, :]

    def x_copy(d):
        to = lax.rem(me_x + d, 4)
        return remote(attv.at[to], att.at[me_x], xs.at[d], xr.at[d], sp, to)

    with jax.named_scope("x_exchange"):
        for d in (2, 1, 3):
            x_copy(d).start()
        for way in range(2):
            down_copy(way).wait()
        for n in range(4):
            pass_on(n)
        att[me_x] = attv[me_x]
        weights[0].wait()
        for d in (1, 3, 2):
            x_copy(d).wait()
    with jax.named_scope("proj"):
        mixed = jnp.zeros(resid_ref.shape, f32)
        for x in range(4):
            mixed = mixed + jnp.dot(att[x], outw[x * LANES:(x + 1) * LANES, :], preferred_element_type=f32)
        residual = (resid_ref[...].astype(f32) + mixed).astype(bf)
        resid_f = residual.astype(f32)
        scale = lax.rsqrt(jnp.mean(resid_f * resid_f, axis=-1, keepdims=True) + eps)
        normed = (resid_f * scale * gain_ref[...]).astype(bf)
        resid_s[...] = residual

    with jax.named_scope("fill"):
        chosen = jnp.dot(pick[...], jnp.concatenate([normed, normed], axis=0), preferred_element_type=f32)
        sendbuf[...] = chosen.astype(bf).reshape(64, 3, 16, LANES)

    def dispatch(dz):
        def send(dj, carry):
            remote(sendbuf.at[dz * 8 + dj], recv.at[dz, dj], ss, sr.at[dz], at_offset(dz, dj), me_x).start()
            return carry

        lax.fori_loop(1 if dz == 0 else 0, 8, send, 0)

    with jax.named_scope("dispatch"):
        for n in PACE[0]:
            dispatch(GROUPS[n])
        recv[0, 0] = sendbuf[0]

    def a_copy(dz, way):
        return remote(
            recv.at[dz], xall.at[2 * way, dz], axs.at[way, dz], axr.at[way, dz], sp, left if way == 0 else right)

    def b_copy(dz, way):
        part = pl.ds(4 * way, 4)
        return remote(
            xall.at[2 * way, dz, part], xall.at[1, dz, part], bxs.at[way, dz], bxr.at[way, dz],
            sp, left if way == 0 else right)

    def h_copy(dz, d):
        return remote(hsend.at[d, dz], hall.at[d, dz], hs.at[d, dz], hr.at[d, dz], sp, lax.rem(me_x + d, 4))

    def stage_a(dz):
        with jax.named_scope(f"A{dz}"):
            arrived = recv.at[0, pl.ds(1, 7)] if dz == 0 else recv.at[dz]
            pltpu.make_async_copy(arrived, arrived, sr.at[dz]).wait()
            for way in range(2):
                a_copy(dz, way).start()
            for n in PACE[GROUPS.index(dz) + 1]:
                dispatch(GROUPS[n])

    def stage_b(dz):
        with jax.named_scope(f"B{dz}"):
            for way in range(2):
                a_copy(dz, way).wait()
                b_copy(dz, way).start()

    def stage_c(pair):
        with jax.named_scope(f"Cw{pair[0]}"):
            for dz in pair:
                for way in range(2):
                    b_copy(dz, way).wait()
        with jax.named_scope(f"C{pair[0]}"):
            block = jnp.concatenate(
                [recv[dz].reshape(24, 16, LANES) for dz in pair]
                + [xall[d, dz].reshape(24, 16, LANES) for d in range(3) for dz in pair], axis=0)
            block = block.reshape(block.shape[0], 16 * LANES)
            gate = jnp.dot(block, gatew[...], preferred_element_type=f32)
            upper = jnp.dot(block, upw[...], preferred_element_type=f32)
            hidden = (gate / (1.0 + jnp.exp(-gate)) * upper).astype(bf)
            for n, dz in enumerate(pair):
                hall[0, dz] = hidden[24 * n:24 * (n + 1)]
                for d in range(1, 4):
                    begin = 24 * (len(pair) * d + n)
                    hsend[d, dz] = hidden[begin:begin + 24]
            for dz in pair:
                for d in range(1, 4):
                    h_copy(dz, d).start()

    def stage_d(pair):
        with jax.named_scope(f"Dw{pair[0]}"):
            for dz in pair:
                for d in range(1, 4):
                    h_copy(dz, d).wait()
        with jax.named_scope(f"D{pair[0]}"):
            full = None
            for d in range(4):
                hidden = jnp.concatenate([hall[d, dz] for dz in pair], axis=0)
                term = jnp.dot(hidden, dcat[(4 - d) % 4], preferred_element_type=f32)
                full = term if full is None else full + term
            tiles = full.astype(bf).reshape(len(pair), 8, 3, 16, LANES)
            for n, dz in enumerate(pair):
                retsend[dz] = tiles[n]
            for dz in pair:
                def give(dj, carry, dz=dz):
                    remote(
                        retsend.at[dz, dj], ret.at[pl.ds(24 * dz + 3 * dj, 3)], ts, tr,
                        at_offset(8 - dz, 8 - dj), me_x).start()
                    return carry

                if dz == 0:
                    ret[0:3] = retsend[0, 0]
                lax.fori_loop(1 if dz == 0 else 0, 8, give, 0)

    def wait_down():
        with jax.named_scope("wait_down"):
            weights[3].wait()
            for way in range(2):
                for n in range(4):
                    down_pass(way, n).wait()

    g = GROUPS
    stage_a(g[0])
    for n in range(1, 11):
        if n < 8:
            stage_a(g[n])
        if n == 2:
            weights[1].wait()
            weights[2].wait()
        if n == 3:
            wait_down()
        if n <= 8:
            stage_b(g[n - 1])
        if 2 <= n <= 9:
            stage_c(g[n - 2:n - 1])
        if 3 <= n:
            stage_d(g[n - 3:n - 2])

    with jax.named_scope("wait_ret"):
        pltpu.make_async_copy(ret.at[pl.ds(3, 189)], ret.at[pl.ds(3, 189)], tr).wait()

    with jax.named_scope("join"):
        picked = jnp.dot(joiner[...], ret[...].reshape(192, 16 * LANES), preferred_element_type=f32)
        share = route_ref[...].T
        both = picked[0:rows] * share[:, 0:1] + picked[rows:] * share[:, 1:2]
        out_ref[...] = (resid_s[...].astype(f32) + both).astype(bf)
    pltpu.make_async_copy(sendbuf.at[pl.ds(1, 63)], sendbuf.at[pl.ds(1, 63)], ss).wait()
    pltpu.make_async_copy(sendbuf.at[pl.ds(1, 63)], sendbuf.at[pl.ds(1, 63)], ts).wait()


def body(
    resid_in,
    query_proj,
    key_proj,
    value_proj,
    query_gain,
    key_gain,
    out_weight,
    norm_gain,
    gate_weight,
    up_weight,
    down_weight,
    expert_ids,
    route_weight,
):
    tok = query_proj.shape[0]
    rows = resid_in.shape[0]
    ff = down_weight.shape[1]
    bf, f32 = jnp.bfloat16, jnp.float32
    dma = pltpu.SemaphoreType.DMA
    vmem = pl.BlockSpec(memory_space=pltpu.VMEM)
    hbm = pl.BlockSpec(memory_space=pl.ANY)
    return pl.pallas_call(
        layer_kernel,
        out_shape=jax.ShapeDtypeStruct(resid_in.shape, bf),
        in_specs=[hbm] * 13,
        out_specs=vmem,
        scratch_shapes=[
            pltpu.VMEM((TOPK, tok), jnp.int32),
            pltpu.VMEM((TOPK, rows), f32),
            pltpu.VMEM(query_proj.shape, bf),
            pltpu.VMEM(key_proj.shape[::-1], bf),
            pltpu.VMEM(value_proj.shape[::-1], bf),
            pltpu.VMEM(query_gain.shape, f32),
            pltpu.VMEM(key_gain.shape, f32),
            pltpu.VMEM(resid_in.shape, bf),
            pltpu.VMEM((1,) + norm_gain.shape, f32),
            dma((9,)),
            pltpu.VMEM((8, tok, LANES), bf),
            pltpu.VMEM((8, tok, LANES), bf),
            pltpu.VMEM((8 * tok, LANES), bf),
            pltpu.VMEM((HEAD_DIM + 16, 8 * tok), bf),
            pltpu.VMEM((8, 1, 2 * tok), f32),
            pltpu.VMEM((8, HEAD_DIM + 16, 2 * tok), f32),
            pltpu.VMEM((8, LANES, tok), bf),
            pltpu.VMEM((8, 2, 2 * tok), f32),
            pltpu.VMEM((8, LANES, tok), bf),
            pltpu.VMEM((8, 2, 2 * tok), f32),
            pltpu.VMEM((4, rows, LANES), bf),
            pltpu.VMEM((4, rows, LANES), bf),
            pltpu.VMEM(out_weight.shape, bf),
            pltpu.VMEM(gate_weight.shape[1:], bf),
            pltpu.VMEM(up_weight.shape[1:], bf),
            pltpu.VMEM((4,) + down_weight.shape[1:], bf),
            pltpu.VMEM((192, TOPK * rows), bf),
            pltpu.VMEM((TOPK * rows, 192), bf),
            pltpu.VMEM(resid_in.shape, bf),
            pltpu.VMEM((64, 3, 16, LANES), bf),
            pltpu.VMEM((8, 8, 3, 16, LANES), bf),
            pltpu.VMEM((3, 8, 8, 3, 16, LANES), bf),
            pltpu.VMEM((4, 8, 24, ff), bf),
            pltpu.VMEM((4, 8, 24, ff), bf),
            pltpu.VMEM((8, 8, 3, 16, LANES), bf),
            pltpu.VMEM((192, 16, LANES), bf),
        ] + [dma((4,))] + [dma((8,))] * 8 + [dma((4,))] * 2 + [dma((10,))] * 2
        + [dma(()), dma((8,))] + [dma((2, 8))] * 4 + [dma((4, 8))] * 2 + [dma(())] * 2,
        compiler_params=pltpu.CompilerParams(
            collective_id=0, has_side_effects=True, vmem_limit_bytes=67_000_000),
    )(
        expert_ids.T, route_weight.T, query_proj, key_proj.T, value_proj.T, query_gain, key_gain, resid_in,
        norm_gain[None], out_weight, gate_weight[0], up_weight[0], down_weight[0],
    )


def solution(mesh):
    placed = (
        P(("sp", "tp"), None),
        P("sp", "tp"),
        P("sp", "tp"),
        P("sp", "tp"),
        P("tp", None),
        P("tp", None),
        P(),
        P(),
        P("sp", None, "tp"),
        P("sp", None, "tp"),
        P("sp", "tp", None),
        P("sp", None),
        P(("sp", "tp"), None),
    )
    return jax.shard_map(
        body, mesh=mesh, in_specs=placed, out_specs=P(("sp", "tp"), None), check_vma=False
    )
```
